32 devices in a mesh: ep: 8 (over z, core), tp: 4 (over y, x).
Axes of the slice: x: 2, y: 2, z: 4, core: 2. Of those that a mesh axis runs over, the one named last changes fastest.
Arguments:
- tokens: bfloat16 [128, 2048], P('ep'), may hold values from -6 to 6
- norm_gain: float32 [2048], replicated, may hold values from 0.1 to 1.9
- w_query: bfloat16 [2048, 512], P('ep', 'tp'), may hold values from -0.125 to 0.125
- w_key: bfloat16 [2048, 512], P('ep', 'tp'), may hold values from -0.125 to 0.125
- w_decay: bfloat16 [2048, 512], P('ep', 'tp'), may hold values from -0.125 to 0.125
- w_value: bfloat16 [2048, 1024], P('ep', 'tp'), may hold values from -0.125 to 0.125
- w_outgate: bfloat16 [2048, 1024], P('ep', 'tp'), may hold values from -0.125 to 0.125
- decay_rate: float32 [512], P('tp'), may hold values from 0.02 to 1
- state: float32 [128, 4, 128, 256], P('ep', 'tp'), may hold values from -15 to 15
- head_gain: float32 [256], replicated, may hold values from 0.1 to 1.9
- w_output: bfloat16 [1024, 2048], P('tp'), may hold values from -0.1875 to 0.1875
- moe_gain: float32 [2048], replicated, may hold values from 0.1 to 1.9
- expert_ids: int32 [128, 2], P('ep'), may hold values from 0 to 7, all different within a row; in each aligned block of 16 rows (0 to 15, 16 to 31, ...) at most 8 rows name the same one
- group_prob: float32 [128], P('ep'), may hold values from 0.3 to 1
- inner_prob: float32 [128, 2], P('ep'), may hold values from 0.05 to 1
- w_gate: bfloat16 [8, 2048, 2048], P('ep', None, 'tp'), may hold values from -0.125 to 0.125
- w_up: bfloat16 [8, 2048, 2048], P('ep', None, 'tp'), may hold values from -0.125 to 0.125
- w_down: bfloat16 [8, 2048, 2048], P('ep', 'tp'), may hold values from -0.125 to 0.125
Outputs:
- output: bfloat16 [128, 2048], P('ep', 'tp')
The draws below stay inside these ranges and needn't reach their ends.
Inputs may be any that keep to these rules, and one draw needn't show every extreme that they name: `expert_ids`: the 2 experts of a token differ. In the rows of one index of ep no expert is named more than 8 times, a bound that some block reaches there.
All inputs are finite; a program needn't handle non-finite values.
Results may differ from the reference program's by a relative error of at most 0.025.
Values may be sent and summed in bfloat16 or wider, within the bound.
No kernel may reach another device: no remote copies, remote signals or barrier semaphores. Data moves between devices by JAX's collectives and lax.ppermute only.
A program may use at most 64 MiB of HBM per device.

```python
import math
import jax
import jax.numpy as jnp
import numpy as np
from jax import lax

D = 2048
DK = 128
DV = 256
GLA_HEADS = 4
FF = 2048
TOP = 2
SEQ_DEV = 16
SEQS = 128
EXPERTS = 8
CAP = 8
FF_BLOCK = 512
N_TP = 4


def shard_levels(key, shape, shards, low, top_value):
    def one(axis_at, shards_of):
        heights = jax.random.uniform(jax.random.fold_in(jax.random.fold_in(key, 6), axis_at), (shards_of,), jnp.float32, low / len(shards), top_value / len(shards))
        return jnp.repeat(jnp.exp(heights), shape[axis_at] // shards_of).reshape((-1,) + (1,) * (len(shape) - axis_at - 1))

    level = one(*shards[0])
    for cut in shards[1:]:
        level = level * one(*cut)
    return level


def routed_block(own_key, own, number, rows, amount, top, bound, lean):
    sequence = jax.random.permutation(own_key, amount)
    heavy_load, usual = shares(amount, rows * top, bound, lean, True), shares(amount, rows * top, bound, lean, False)
    places = jnp.arange(amount)

    def named(sizes, rotation):
        used = int((sizes > 0).sum())
        fixed = max(1, used // 4)
        passed = fixed + (places - fixed + rotation * (used - fixed)) % max(1, amount - fixed)
        return jnp.zeros((amount,), jnp.int32).at[sequence[jnp.where(places < fixed, places, passed)]].set(jnp.asarray(sizes, jnp.int32))

    sizes = jnp.where(number % 4 == 0, named(heavy_load, number // 4), named(usual, number - number // 4 - 1))
    mixed = jax.random.permutation(jax.random.fold_in(own, 3), amount)
    source_of, receiver = mixed[0:amount // 2 * 2:2], mixed[1:amount // 2 * 2:2]
    slack = jnp.minimum(sizes[source_of] - 1, bound - sizes[receiver]) // 2
    slack = jnp.where((source_of == sequence[0]) | (receiver == sequence[0]) | (sizes[receiver] == 0), 0, jnp.maximum(slack, 0))
    passed = jax.random.randint(jax.random.fold_in(own, 4), (amount // 2,), 0, 1 << 20) % (slack + 1)
    sizes = sizes.at[source_of].add(-passed).at[receiver].add(passed)
    items = jnp.searchsorted(jnp.cumsum(sizes), jnp.arange(rows * top), side="right").astype(jnp.int32)
    listing = items.reshape(top, rows).T
    listing = listing[jax.random.permutation(jax.random.fold_in(own, 1), rows)]
    rotation = jax.random.randint(jax.random.fold_in(own, 2), (rows, 1), 0, top)
    return jnp.take_along_axis(listing, (jnp.arange(top)[None, :] + rotation) % top, axis=1)


def shares(count, total, reach, skew, full):
    weights = [(1 << 20) // math.isqrt(standing ** skew) + 1 for standing in range(1, count + 1)]
    largest = reach if full else min(reach, max(-(-total // count), total * weights[0] // sum(weights)))
    least = 1 if total - largest >= count - 1 else 0
    holding, rest = [largest] + [least] * (count - 1), total - largest - least * (count - 1)
    while rest > 0:
        movable = [i for i in range(1, count) if holding[i] < largest] or [i for i in range(1, count) if holding[i] < reach]
        mass, budget = sum([weights[i] for i in movable]), rest
        for i in movable:
            addition = min(reach - holding[i], max(1, budget * weights[i] // mass), rest)
            holding[i] = holding[i] + addition
            rest = rest - addition
    return np.array(holding)


def scatter_about(rng, extent, width, limit, split=(), kind=jnp.bfloat16):
    result = width * jax.random.normal(rng, extent, jnp.float32)
    if split:
        result = result * shard_levels(rng, extent, split, -0.22, 0.18)
    return jnp.clip(result, -limit, limit).astype(kind)


def setup_inputs(seed: int = 0) -> dict:
    streams_of = jax.random.split(jax.random.key(seed), 19)
    tokens = scatter_about(streams_of[0], (SEQS, D), 1.0, 6.0, ((0, 8),))
    norm_gain = jnp.clip(1.0 + 0.18 * jax.random.normal(streams_of[1], (D,), jnp.float32), 0.1, 1.9)
    w_query = scatter_about(streams_of[2], (D, GLA_HEADS * DK), D ** -0.5, 0.125, ((0, 8), (1, 4)))
    w_key = scatter_about(streams_of[3], (D, GLA_HEADS * DK), D ** -0.5, 0.125, ((0, 8), (1, 4)))
    w_decay = scatter_about(streams_of[4], (D, GLA_HEADS * DK), D ** -0.5, 0.125, ((0, 8), (1, 4)))
    w_value = scatter_about(streams_of[5], (D, GLA_HEADS * DV), D ** -0.5, 0.125, ((0, 8), (1, 4)))
    w_outgate = scatter_about(streams_of[6], (D, GLA_HEADS * DV), D ** -0.5, 0.125, ((0, 8), (1, 4)))
    decay_rate = jnp.clip(jnp.exp(math.log(1.0) - 3.912023 * jax.random.uniform(streams_of[7], (GLA_HEADS * DK,), jnp.float32) ** shard_levels(streams_of[7], (GLA_HEADS * DK,), ((0, 4),), -0.2, 0.2)), 0.02, 1.0)
    state = scatter_about(streams_of[8], (SEQS, GLA_HEADS, DK, DV), 3.0, 15.0, ((0, 8), (1, 4)), jnp.float32)
    head_gain = jnp.clip(1.0 + 0.18 * jax.random.normal(streams_of[9], (DV,), jnp.float32), 0.1, 1.9)
    w_output = scatter_about(streams_of[10], (GLA_HEADS * DV, D), (GLA_HEADS * DV) ** -0.5, 0.1875, ((0, 4),))
    moe_gain = jnp.clip(1.0 + 0.18 * jax.random.normal(streams_of[11], (D,), jnp.float32), 0.1, 1.9)
    expert_ids_keys = jax.random.split(jax.random.fold_in(streams_of[12], 1), SEQS // SEQ_DEV)
    expert_ids_turns = jax.random.permutation(jax.random.fold_in(streams_of[12], 3), SEQS // SEQ_DEV)
    expert_ids = jax.vmap(lambda own, number: routed_block(jax.random.fold_in(streams_of[12], 2), own, number, SEQ_DEV, EXPERTS, TOP, CAP, 2))(expert_ids_keys, expert_ids_turns).reshape((SEQS, TOP))
    group_prob = jnp.clip(0.3 + 0.7 * jax.random.uniform(streams_of[13], (SEQS,), jnp.float32) ** shard_levels(streams_of[13], (SEQS,), ((0, 8),), -0.2, 0.2), 0.3, 1.0)
    inner_prob = jnp.clip(0.05 + 0.95 * jax.random.uniform(streams_of[14], (SEQS, TOP), jnp.float32) ** shard_levels(streams_of[14], (SEQS, TOP), ((0, 8),), -0.2, 0.2), 0.05, 1.0)
    w_gate = scatter_about(streams_of[15], (EXPERTS, D, FF), D ** -0.5, 0.125, ((0, 8), (2, 4)))
    w_up = scatter_about(streams_of[16], (EXPERTS, D, FF), D ** -0.5, 0.125, ((0, 8), (2, 4)))
    w_down = scatter_about(streams_of[17], (EXPERTS, FF, D), FF ** -0.5, 0.125, ((0, 8), (1, 4)))
    return {"tokens": tokens, "norm_gain": norm_gain, "w_query": w_query, "w_key": w_key, "w_decay": w_decay, "w_value": w_value, "w_outgate": w_outgate, "decay_rate": decay_rate, "state": state, "head_gain": head_gain, "w_output": w_output, "moe_gain": moe_gain, "expert_ids": expert_ids, "group_prob": group_prob, "inner_prob": inner_prob, "w_gate": w_gate, "w_up": w_up, "w_down": w_down}


epsilon = 1e-05

def inverse_rms(values):
    return lax.rsqrt(lax.optimization_barrier(jnp.mean(values * values, axis=-1, keepdims=True)) + epsilon)

def reference(tokens, norm_gain, w_query, w_key, w_decay, w_value, w_outgate, decay_rate, state, head_gain, w_output, moe_gain, expert_ids, group_prob, inner_prob, w_gate, w_up, w_down):
    wide = jnp.float32
    narrow = jnp.bfloat16
    residual = tokens.astype(wide)
    normed = (residual * inverse_rms(residual) * norm_gain.astype(wide)).astype(narrow)

    def project(weight):
        return jnp.dot(normed, weight, preferred_element_type=wide)
    query = project(w_query).astype(narrow).astype(wide).reshape(SEQS, GLA_HEADS, DK) * DK ** (-0.5)
    key_rows = project(w_key).astype(narrow).astype(wide).reshape(SEQS, GLA_HEADS, DK)
    value_rows = project(w_value).astype(narrow).astype(wide).reshape(SEQS, GLA_HEADS, DV)
    gate_rows = project(w_outgate).astype(narrow).astype(wide).reshape(SEQS, GLA_HEADS, DV)
    decay_log = jax.nn.log_sigmoid(project(w_decay)) * decay_rate
    decay = jnp.exp(decay_log).reshape(SEQS, GLA_HEADS, DK)
    updated = decay[..., None] * state + key_rows[..., None] * value_rows[:, :, None, :]
    readout = jnp.einsum('shk,shkv->shv', query, updated, precision=lax.Precision.HIGHEST)
    gated = (readout * inverse_rms(readout) * head_gain.astype(wide) * jax.nn.silu(gate_rows)).astype(narrow)
    per_head = jnp.einsum('shv,hvd->shd', gated.astype(wide), w_output.astype(wide).reshape(GLA_HEADS, DV, D))
    attention = lax.optimization_barrier(jnp.sum(per_head.astype(narrow).astype(wide), axis=1))
    mixed = (residual + attention).astype(narrow)
    mixed_wide = mixed.astype(wide)
    moe_in = (mixed_wide * inverse_rms(mixed_wide) * moe_gain.astype(wide)).astype(narrow)
    route_weight = group_prob[:, None] * inner_prob / lax.optimization_barrier(jnp.sum(inner_prob, axis=1, keepdims=True))
    slot_total = EXPERTS * CAP

    def one_expert(total, inputs):
        weight_gate, weight_up, weight_down, index = inputs
        chosen = expert_ids == index
        coeff = lax.optimization_barrier(jnp.sum(jnp.where(chosen, route_weight, 0.0), axis=1))
        marks = jnp.where(jnp.any(chosen, axis=1), 0, 1).astype(jnp.int32)
        order = jnp.argsort(marks, stable=True)[:slot_total].astype(jnp.int32)
        rows = moe_in[order]
        gate = jnp.dot(rows, weight_gate, preferred_element_type=wide)
        upper = jnp.dot(rows, weight_up, preferred_element_type=wide)
        hidden = (jax.nn.silu(gate) * upper).astype(narrow)
        pieces = jnp.einsum('rbf,bfd->rbd', hidden.astype(wide).reshape(slot_total, N_TP, FF_BLOCK), weight_down.astype(wide).reshape(N_TP, FF_BLOCK, D))
        expert_out = lax.optimization_barrier(jnp.sum(pieces.astype(narrow).astype(wide), axis=1)).astype(narrow).astype(wide)
        total = total.at[order].add(coeff[order][:, None] * expert_out)
        return (total, None)
    experts_sum, _ = lax.scan(one_expert, jnp.zeros((SEQS, D), wide), (w_gate, w_up, w_down, jnp.arange(EXPERTS, dtype=jnp.int32)))
    return (mixed_wide + experts_sum).astype(narrow)
```

```python
import jax
import jax.numpy as jnp
from jax import lax
from jax.sharding import PartitionSpec as P

epsilon = 1e-05
wide = jnp.float32
narrow = jnp.bfloat16


def inverse_rms(values):
    return lax.rsqrt(jnp.mean(values * values, axis=-1, keepdims=True) + epsilon)


def swap_core(block):
    count = lax.axis_size("ep")
    return lax.ppermute(block, "ep", [(i, i ^ 1) for i in range(count)])


def swap_chip(block, step):
    count = lax.axis_size("ep")
    return lax.ppermute(block, "ep", [(i, i ^ (2 * step)) for i in range(count)])


def swap_head(block, step):
    count = lax.axis_size("tp")
    return lax.ppermute(block, "tp", [(i, i ^ step) for i in range(count)])


def on_device(
    tokens,
    norm_gain,
    w_query,
    w_key,
    w_decay,
    w_value,
    w_outgate,
    decay_rate,
    state,
    head_gain,
    w_output,
    moe_gain,
    expert_ids,
    group_prob,
    inner_prob,
    w_gate,
    w_up,
    w_down,
):
    seqs, width = tokens.shape
    ep_count, tp_count = lax.axis_size("ep"), lax.axis_size("tp")
    chips = ep_count // 2
    heads, key_width, value_width = state.shape[1:]
    me, head = lax.axis_index("ep"), lax.axis_index("tp")
    chip, core = me // 2, me % 2
    feats = width // ep_count
    residual = tokens.astype(wide)

    pair_cols = [
        lax.dynamic_slice_in_dim(tokens, (chip ^ k) * 2 * feats, 2 * feats, 1) for k in range(chips)
    ]
    gathered = jnp.concatenate(
        [pair_cols[0]] + [swap_chip(pair_cols[k], k) for k in range(1, chips)], axis=0
    )
    keep = lax.dynamic_slice_in_dim(gathered, core * feats, feats, 1)
    away = lax.dynamic_slice_in_dim(gathered, (1 - core) * feats, feats, 1)
    rows = jnp.concatenate([keep, swap_core(away)], axis=0)
    gain = lax.dynamic_slice_in_dim(norm_gain, me * feats, feats, 0)
    rows = (rows.astype(wide) * gain).astype(narrow)
    weights = jnp.concatenate([w_query, w_key, w_decay, w_value, w_outgate], axis=1)
    partial = jnp.dot(rows, weights, preferred_element_type=wide)
    half = chips * seqs
    both = partial[:half] + swap_core(partial[half:].astype(narrow)).astype(wide)
    both_narrow = both.astype(narrow)
    projected = both[:seqs]
    for k in range(chips - 1, 0, -1):
        projected = projected + swap_chip(both_narrow[k * seqs : (k + 1) * seqs], k).astype(wide)
    projected = projected * inverse_rms(residual)

    query_cols, value_cols = w_query.shape[1], w_value.shape[1]
    rounded = projected.astype(narrow).astype(wide)
    query = rounded[:, :query_cols].reshape(seqs, heads, key_width) * key_width ** (-0.5)
    key_rows = rounded[:, query_cols : 2 * query_cols].reshape(seqs, heads, key_width)
    decay_pre = projected[:, 2 * query_cols : 3 * query_cols]
    value_rows = rounded[:, 3 * query_cols : 3 * query_cols + value_cols]
    value_rows = value_rows.reshape(seqs, heads, value_width)
    gate_rows = rounded[:, 3 * query_cols + value_cols :].reshape(seqs, heads, value_width)
    decay = jnp.exp(jax.nn.log_sigmoid(decay_pre) * decay_rate).reshape(seqs, heads, key_width)
    readout = jnp.sum((query * decay)[..., None] * state, axis=2) + (
        jnp.sum(query * key_rows, axis=-1, keepdims=True) * value_rows
    )
    gated = (readout * inverse_rms(readout) * head_gain * jax.nn.silu(gate_rows)).astype(narrow)
    head_part = jnp.dot(
        gated.reshape(seqs, heads * value_width), w_output, preferred_element_type=wide
    ).astype(narrow)
    attention = head_part.astype(wide)
    for k in range(tp_count - 1, 0, -1):
        attention = attention + swap_head(head_part, k).astype(wide)
    mixed_wide = (residual + attention).astype(narrow).astype(wide)
    moe_in = (mixed_wide * inverse_rms(mixed_wide) * moe_gain).astype(narrow)

    route_weight = group_prob[:, None] * inner_prob / jnp.sum(inner_prob, axis=1, keepdims=True)
    expert_range = jnp.arange(ep_count, dtype=jnp.int32)
    share = jnp.sum(
        jnp.where(expert_ids[:, :, None] == expert_range, route_weight[:, :, None], 0.0), axis=1
    )
    share_high = lax.reduce_precision(share, 8, 7)
    share_low = lax.reduce_precision(share - share_high, 8, 7)
    lanes = -(-2 * ep_count // 128) * 128
    share_packed = jnp.concatenate(
        [share_high, share_low, jnp.zeros((seqs, lanes - 2 * ep_count), wide)], axis=1
    ).astype(narrow)
    sending = jnp.concatenate([moe_in, share_packed], axis=1)
    arrived = jnp.concatenate(
        [sending] + [swap_chip(sending, k) for k in range(1, chips)], axis=0
    )
    arrived = jnp.concatenate([arrived, swap_core(arrived)], axis=0)
    row_in = arrived[:, :width]
    share_all = arrived[:, width:].astype(wide)
    mine = jnp.sum(
        jnp.where(jnp.arange(lanes) % ep_count == me, share_all, 0.0), axis=1, keepdims=True
    )
    gate = jnp.dot(row_in, w_gate[0], preferred_element_type=wide)
    upper = jnp.dot(row_in, w_up[0], preferred_element_type=wide)
    hidden = (jax.nn.silu(gate) * upper).astype(narrow)
    block_out = jnp.dot(hidden, w_down[0], preferred_element_type=wide) * mine

    pair_sum = block_out[:half] + swap_core(block_out[half:].astype(narrow)).astype(wide)
    pair_sum = pair_sum.astype(narrow)
    cols = width // tp_count
    pieces = [
        lax.dynamic_slice_in_dim(pair_sum, (head ^ k) * cols, cols, 1) for k in range(tp_count)
    ]
    head_sum = pieces[0].astype(wide)
    for k in range(tp_count - 1, 0, -1):
        head_sum = head_sum + swap_head(pieces[k], k).astype(wide)
    head_narrow = head_sum.astype(narrow)
    moe_sum = head_sum[:seqs]
    for k in range(chips - 1, 0, -1):
        moe_sum = moe_sum + swap_chip(head_narrow[k * seqs : (k + 1) * seqs], k).astype(wide)
    own_cols = lax.dynamic_slice_in_dim(mixed_wide, head * cols, cols, 1)
    return (own_cols + moe_sum).astype(narrow)


def solution(mesh):
    placed = (
        P("ep", None),
        P(),
        P("ep", "tp"),
        P("ep", "tp"),
        P("ep", "tp"),
        P("ep", "tp"),
        P("ep", "tp"),
        P("tp"),
        P("ep", "tp", None, None),
        P(),
        P("tp", None),
        P(),
        P("ep", None),
        P("ep"),
        P("ep", None),
        P("ep", None, "tp"),
        P("ep", None, "tp"),
        P("ep", "tp", None),
    )
    return jax.shard_map(
        on_device, mesh=mesh, in_specs=placed, out_specs=P("ep", "tp"), check_vma=False
    )
```

```python
import functools

import jax
import jax.numpy as jnp
from jax import lax
from jax.experimental import pallas as pl
from jax.experimental.pallas import tpu as pltpu
from jax.sharding import PartitionSpec as P


epsilon = 1e-05
wide = jnp.float32
narrow = jnp.bfloat16
lane_tile = 128


def inverse_rms(values):
    return lax.rsqrt(jnp.mean(values * values, axis=-1, keepdims=True) + epsilon)


def silu(values):
    return values / (1.0 + jnp.exp(-values))


def swap_core(block):
    count = lax.axis_size("ep")
    return lax.ppermute(block, "ep", [(i, i ^ 1) for i in range(count)])


def swap_chips(blocks):
    count = lax.axis_size("ep")
    got = {}
    for k in range(len(blocks) - 1, 0, -1):
        got[k] = lax.ppermute(blocks[k], "ep", [(i, i ^ (2 * k + 1)) for i in range(count)])
    return [got[k] for k in range(1, len(blocks))]


def swap_heads(blocks, other_core):
    ep_count, count = lax.axis_size("ep"), lax.axis_size("tp")
    got = {}
    for k in range(len(blocks) - 1, 0, -1):
        pairs = [
            (e * count + t, (e ^ other_core) * count + (t ^ k))
            for e in range(ep_count)
            for t in range(count)
        ]
        got[k] = lax.ppermute(blocks[k], ("ep", "tp"), pairs)
    return [got[k] for k in range(1, len(blocks))]


def call(kernel, outs, args, limit, flops=0):
    nbytes = sum(a.size * a.dtype.itemsize for a in args)
    nbytes += sum(o.size * o.dtype.itemsize for o in outs)
    return pl.pallas_call(
        kernel,
        out_shape=tuple(outs),
        in_specs=[pl.BlockSpec(memory_space=pltpu.VMEM)] * len(args),
        out_specs=tuple(pl.BlockSpec(memory_space=pltpu.VMEM) for _ in outs),
        compiler_params=pltpu.CompilerParams(vmem_limit_bytes=limit),
        cost_estimate=pl.CostEstimate(flops=flops, bytes_accessed=nbytes, transcendentals=0),
    )(*args)


def load_call(kernel, args, extra):
    outs = [like(a.shape, a.dtype) for a in args] + list(extra)
    return pl.pallas_call(
        functools.partial(kernel, len(args)),
        out_shape=tuple(outs),
        in_specs=[pl.BlockSpec(memory_space=pltpu.HBM)] * len(args),
        out_specs=tuple(pl.BlockSpec(memory_space=pltpu.VMEM) for _ in outs),
        scratch_shapes=[pltpu.SemaphoreType.DMA((len(args),))],
        compiler_params=pltpu.CompilerParams(vmem_limit_bytes=2 << 20),
        cost_estimate=pl.CostEstimate(flops=1 << 22, bytes_accessed=1 << 22, transcendentals=0),
    )(*[pltpu.with_memory_space_constraint(a, pltpu.HBM) for a in args])


def like(shape, dtype):
    return jax.ShapeDtypeStruct(shape, dtype)


def spread_kernel(tokens_ref, *out_refs):
    chip = lax.axis_index("ep") // 2
    cols = out_refs[0].shape[1]
    for k, out in enumerate(out_refs):
        out[...] = tokens_ref[:, pl.ds(pl.multiple_of((chip ^ k) * cols, lane_tile), cols)]


def load(pairs, sems):
    copies = [pltpu.make_async_copy(src, dst, sems.at[n]) for n, (src, dst) in enumerate(pairs)]
    for copy in copies:
        copy.start()
    return copies


def load_kernel(count, *refs):
    for copy in load(list(zip(refs[:count], refs[count : 2 * count])), refs[-1]):
        copy.wait()


def side_kernel(count, *refs):
    loaded = refs[count : 2 * count]
    scale_ref, share_ref, sems = refs[2 * count :]
    copies = load(list(zip(refs[:count], loaded)), sems)
    for copy in copies[:4]:
        copy.wait()
    tokens_ref, ids_ref, group_ref, inner_ref = loaded[:4]
    experts = lax.axis_size("ep")
    scale_ref[...] = jnp.broadcast_to(inverse_rms(tokens_ref[...].astype(wide)), scale_ref.shape)
    lanes, seqs = share_ref.shape[1], share_ref.shape[0]
    inner = inner_ref[...]
    weight = group_ref[...] * inner / jnp.sum(inner, axis=0, keepdims=True)
    place = lax.broadcasted_iota(jnp.int32, (lanes, seqs), 0)
    owner = jnp.where(place >= experts, place - experts, place)
    share = jnp.zeros((lanes, seqs), wide)
    for k in range(ids_ref.shape[0]):
        share = share + jnp.where(owner == ids_ref[k : k + 1, :], weight[k : k + 1, :], 0.0)
    high = share.astype(narrow).astype(wide)
    packed = jnp.where(place < experts, high, jnp.where(place < 2 * experts, share - high, 0.0))
    share_ref[...] = packed.T.astype(narrow)
    for copy in copies[4:]:
        copy.wait()


def project_kernel(chips, gain_ref, *refs):
    blocks, refs = refs[: 2 * chips], refs[2 * chips :]
    weights, (own_ref, away_ref) = refs[:-2], refs[-2:]
    me = lax.axis_index("ep")
    south = me % 2 == 0
    feats = weights[0].shape[0]
    pair_gain = gain_ref[:, pl.ds(pl.multiple_of(me // 2 * 2 * feats, lane_tile), 2 * feats)]
    rows = jnp.concatenate([block[...] for block in blocks], axis=0).astype(wide) * pair_gain
    rows = jnp.where(south, rows[:, :feats], rows[:, feats:]).astype(narrow)
    half = own_ref.shape[0]
    at = 0
    for weight in weights:
        cols = weight.shape[1]
        product = jnp.dot(rows, weight[...], preferred_element_type=wide)
        own_ref[:, at : at + cols] = product[:half]
        away_ref[:, at : at + cols] = product[half:].astype(narrow)
        at += cols


def recurrent_kernel(chips, cuts, base_ref, *refs):
    arrived, refs = refs[: chips - 1], refs[chips - 1 :]
    scale_ref, rate_ref, state_ref, gain_ref, output_ref, part_ref, read_ref = refs
    query_cols, value_cols = cuts
    seqs, heads, key_width, value_width = state_ref.shape
    total = base_ref[...]
    for block in arrived:
        total = total + block[...].astype(wide)
    total = total * scale_ref[:, :1]
    rounded = total.astype(narrow).astype(wide)
    pre = total[:, 2 * query_cols : 3 * query_cols]
    log_gate = jnp.minimum(pre, 0.0) - jnp.log1p(jnp.exp(-jnp.abs(pre)))
    decay = jnp.exp(log_gate * rate_ref[...])
    query = rounded[:, :query_cols] * key_width ** (-0.5)
    keys = rounded[:, query_cols : 2 * query_cols]
    turned = (query * decay).T
    out = None
    for h in range(heads):
        span = slice(h * key_width, (h + 1) * key_width)
        at = 3 * query_cols + h * value_width
        values = rounded[:, at : at + value_width]
        gates = rounded[:, at + value_cols : at + value_cols + value_width]
        for s in range(seqs):
            column = turned[span, s : s + 1]
            read_ref[s : s + 1, :] = jnp.sum(column * state_ref[s, h], axis=0, keepdims=True)
        match = jnp.sum(query[:, span] * keys[:, span], axis=1, keepdims=True)
        readout = read_ref[...] + match * values
        gated = (readout * inverse_rms(readout) * gain_ref[...] * silu(gates)).astype(narrow)
        rows = slice(h * value_width, (h + 1) * value_width)
        part = jnp.dot(gated, output_ref[rows, :], preferred_element_type=wide)
        out = part if out is None else out + part
    part_ref[...] = out.astype(narrow)


def mix_kernel(others, tokens_ref, part_ref, *refs):
    arrived, (gain_ref, share_ref, send_ref, own_ref) = refs[:others], refs[others:]
    width = tokens_ref.shape[1]
    attention = part_ref[...].astype(wide)
    for block in arrived:
        attention = attention + block[...].astype(wide)
    mixed = (tokens_ref[...].astype(wide) + attention).astype(narrow).astype(wide)
    send_ref[:, :width] = (mixed * inverse_rms(mixed) * gain_ref[...]).astype(narrow)
    send_ref[:, width:] = share_ref[...]
    cols = own_ref.shape[1]
    head = lax.axis_index("tp")
    attention = jnp.zeros(own_ref.shape, wide)
    at = pl.ds(pl.multiple_of(head * cols, lane_tile), cols)
    for block in (part_ref, *arrived):
        attention = attention + block[:, at].astype(wide)
    own_ref[...] = (tokens_ref[:, at].astype(wide) + attention).astype(narrow).astype(wide)


def expert_kernel(count, *refs):
    blocks, (gate_ref, up_ref, down_ref, own_ref, away_ref) = refs[:count], refs[count:]
    width = gate_ref.shape[1]
    rows = jnp.concatenate([block[:, :width] for block in blocks], axis=0)
    share = jnp.concatenate([block[:, width:] for block in blocks], axis=0).astype(wide)
    me, experts = lax.axis_index("ep"), lax.axis_size("ep")
    place = lax.broadcasted_iota(jnp.int32, share.shape, 1)
    chosen = (place == me) | (place == me + experts)
    weight = jnp.sum(jnp.where(chosen, share, 0.0), axis=1, keepdims=True)
    gate = jnp.dot(rows, gate_ref[0], preferred_element_type=wide)
    upper = jnp.dot(rows, up_ref[0], preferred_element_type=wide)
    hidden = (silu(gate) * upper).astype(narrow)
    head = lax.axis_index("tp")
    pieces, half, cols = own_ref.shape
    for k in range(pieces):
        at = pl.ds(pl.multiple_of((head ^ k) * cols, lane_tile), cols)
        out = jnp.dot(hidden, down_ref[0, :, at], preferred_element_type=wide) * weight
        near, far = (out[:half], out[half:]) if k == 0 else (out[half:], out[:half])
        own_ref[k] = near
        away_ref[k] = far.astype(narrow)


def on_device(
    tokens,
    norm_gain,
    w_query,
    w_key,
    w_decay,
    w_value,
    w_outgate,
    decay_rate,
    state,
    head_gain,
    w_output,
    moe_gain,
    expert_ids,
    group_prob,
    inner_prob,
    w_gate,
    w_up,
    w_down,
):
    seqs, width = tokens.shape
    ep_count, tp_count = lax.axis_size("ep"), lax.axis_size("tp")
    chips = ep_count // 2
    half = chips * seqs
    _, _, value_width = state.shape[1:]
    feats = w_query.shape[0]
    query_cols, value_cols = w_query.shape[1], w_value.shape[1]
    proj_cols = 3 * query_cols + 2 * value_cols
    cols = width // tp_count
    lanes = -(-2 * ep_count // lane_tile) * lane_tile
    mib = 1 << 20

    pair_cols = call(spread_kernel, [like((seqs, 2 * feats), narrow)] * chips, (tokens,), 4 * mib)
    blocks = [pair_cols[0], *swap_chips(pair_cols)]
    blocks += [swap_core(block) for block in blocks]
    side_args = (
        tokens,
        expert_ids.T,
        group_prob[None, :],
        inner_prob.T,
        norm_gain[None, :],
        w_query,
        w_key,
        w_decay,
        w_value,
        w_outgate,
        decay_rate[None, :],
        head_gain[None, :],
        moe_gain[None, :],
        w_output,
        state,
    )
    loaded = load_call(
        side_kernel, side_args, [like((seqs, lane_tile), wide), like((seqs, lanes), narrow)]
    )
    tokens_near = loaded[0]
    gain, weights = loaded[4], loaded[5:10]
    rate, read_gain, mix_gain, output_near, state_near, scale, share = loaded[10:]
    own, away = call(
        functools.partial(project_kernel, chips),
        [like((half, proj_cols), wide), like((half, proj_cols), narrow)],
        (gain, *blocks, *weights),
        8 * mib,
    )
    both = own + swap_core(away).astype(wide)
    both_narrow = both.astype(narrow)
    arrived = swap_chips([both_narrow[k * seqs : (k + 1) * seqs] for k in range(chips)])
    expert_weights = load_call(load_kernel, (w_gate, w_up, w_down), [])
    (part,) = pl.pallas_call(
        functools.partial(recurrent_kernel, chips, (query_cols, value_cols)),
        out_shape=(like((seqs, width), narrow),),
        in_specs=[pl.BlockSpec(memory_space=pltpu.VMEM)] * (chips + 5),
        out_specs=(pl.BlockSpec(memory_space=pltpu.VMEM),),
        scratch_shapes=[pltpu.VMEM((seqs, value_width), wide)],
        compiler_params=pltpu.CompilerParams(vmem_limit_bytes=8 * mib),
        cost_estimate=pl.CostEstimate(flops=1 << 20, bytes_accessed=4 << 20, transcendentals=0),
        name="recurrent",
    )(both[:seqs], *arrived, scale, rate, state_near, read_gain, output_near)
    parts = swap_heads([part] * tp_count, 0)
    sending, mixed_own = call(
        functools.partial(mix_kernel, tp_count - 1),
        [like((seqs, width + lanes), narrow), like((seqs, cols), wide)],
        (tokens_near, part, *parts, mix_gain, share),
        4 * mib,
    )
    rows = [sending, *swap_chips([sending] * chips)]
    rows += [swap_core(block) for block in rows]
    own, away = call(
        functools.partial(expert_kernel, 2 * chips),
        [like((tp_count, half, cols), wide), like((tp_count, half, cols), narrow)],
        (*rows, *expert_weights),
        24 * mib,
    )
    pair_sum = own + swap_core(away).astype(wide)
    pair_narrow = pair_sum.astype(narrow)
    head_sum = pair_sum[0]
    for block in swap_heads([pair_narrow[k] for k in range(tp_count)], 1):
        head_sum = head_sum + block.astype(wide)
    head_narrow = head_sum.astype(narrow)
    moe_sum = head_sum[:seqs]
    for block in swap_chips([head_narrow[k * seqs : (k + 1) * seqs] for k in range(chips)]):
        moe_sum = moe_sum + block.astype(wide)
    return (mixed_own + moe_sum).astype(narrow)


def solution(mesh):
    placed = (
        P("ep", None),
        P(),
        P("ep", "tp"),
        P("ep", "tp"),
        P("ep", "tp"),
        P("ep", "tp"),
        P("ep", "tp"),
        P("tp"),
        P("ep", "tp", None, None),
        P(),
        P("tp", None),
        P(),
        P("ep", None),
        P("ep"),
        P("ep", None),
        P("ep", None, "tp"),
        P("ep", None, "tp"),
        P("ep", "tp", None),
    )

    return jax.shard_map(
        on_device, mesh=mesh, in_specs=placed, out_specs=P("ep", "tp"), check_vma=False
    )
```

```python
import functools

import jax
import jax.numpy as jnp
from jax import lax
from jax.experimental import pallas as pl
from jax.experimental.pallas import tpu as pltpu
from jax.sharding import PartitionSpec as P


epsilon = 1e-05
wide = jnp.float32
narrow = jnp.bfloat16
lane_tile = 128


def inverse_rms(values):
    return lax.rsqrt(jnp.mean(values * values, axis=-1, keepdims=True) + epsilon)


def silu(values):
    return values / (1.0 + jnp.exp(-values))


def swap_core(block):
    count = lax.axis_size("ep")
    return lax.ppermute(block, "ep", [(i, i ^ 1) for i in range(count)])


def swap_chips(blocks):
    count = lax.axis_size("ep")
    got = {}
    for k in range(len(blocks) - 1, 0, -1):
        got[k] = lax.ppermute(blocks[k], "ep", [(i, i ^ (2 * k + 1)) for i in range(count)])
    return [got[k] for k in range(1, len(blocks))]


def swap_heads(blocks, other_core):
    ep_count, count = lax.axis_size("ep"), lax.axis_size("tp")
    got = {}
    for k in range(len(blocks) - 1, 0, -1):
        pairs = [
            (e * count + t, (e ^ other_core) * count + (t ^ k))
            for e in range(ep_count)
            for t in range(count)
        ]
        got[k] = lax.ppermute(blocks[k], ("ep", "tp"), pairs)
    return [got[k] for k in range(1, len(blocks))]


def call(kernel, outs, args, limit, flops=0):
    nbytes = sum(a.size * a.dtype.itemsize for a in args)
    nbytes += sum(o.size * o.dtype.itemsize for o in outs)
    return pl.pallas_call(
        kernel,
        out_shape=tuple(outs),
        in_specs=[pl.BlockSpec(memory_space=pltpu.VMEM)] * len(args),
        out_specs=tuple(pl.BlockSpec(memory_space=pltpu.VMEM) for _ in outs),
        compiler_params=pltpu.CompilerParams(vmem_limit_bytes=limit),
        cost_estimate=pl.CostEstimate(flops=flops, bytes_accessed=nbytes, transcendentals=0),
    )(*args)


def load_call(kernel, args, outs, copies, near=()):
    return pl.pallas_call(
        kernel,
        out_shape=tuple(outs),
        in_specs=[pl.BlockSpec(memory_space=pltpu.VMEM)] * len(near)
        + [pl.BlockSpec(memory_space=pltpu.HBM)] * len(args),
        out_specs=tuple(pl.BlockSpec(memory_space=pltpu.VMEM) for _ in outs),
        scratch_shapes=[pltpu.SemaphoreType.DMA((copies,))],
        compiler_params=pltpu.CompilerParams(vmem_limit_bytes=2 << 20),
        cost_estimate=pl.CostEstimate(flops=1 << 22, bytes_accessed=1 << 22, transcendentals=0),
    )(*near, *[pltpu.with_memory_space_constraint(a, pltpu.HBM) for a in args])


def like(shape, dtype):
    return jax.ShapeDtypeStruct(shape, dtype)


def load(pairs, sems):
    copies = [pltpu.make_async_copy(src, dst, sems.at[n]) for n, (src, dst) in enumerate(pairs)]
    for copy in copies:
        copy.start()
    return copies


def load_kernel(count, *refs):
    for copy in load(list(zip(refs[:count], refs[count : 2 * count])), refs[-1]):
        copy.wait()


def spread_kernel(weights, *refs):
    tokens_ref, weight_refs, refs = refs[0], refs[1 : 1 + weights], refs[1 + weights :]
    *block_refs, near_ref, joined_ref, sems = refs
    chip = lax.axis_index("ep") // 2
    cols = block_refs[0].shape[1]
    pairs = []
    for k in range(len(block_refs) - 1, -1, -1):
        at = pl.ds(pl.multiple_of((chip ^ k) * cols, lane_tile), cols)
        pairs.append((tokens_ref.at[:, at], block_refs[k]))
    pairs.append((tokens_ref, near_ref))
    at = 0
    for weight in weight_refs:
        pairs.append((weight, joined_ref.at[:, at : at + weight.shape[1]]))
        at += weight.shape[1]
    for copy in load(pairs, sems):
        copy.wait()


def side_kernel(count, *refs):
    tokens_ref, refs = refs[0], refs[1:]
    loaded = refs[count : 2 * count]
    scale_ref, share_ref, sems = refs[2 * count :]
    copies = load(list(zip(refs[:count], loaded)), sems)
    scale_ref[...] = jnp.broadcast_to(inverse_rms(tokens_ref[...].astype(wide)), scale_ref.shape)
    for copy in copies[:3]:
        copy.wait()
    ids_ref, group_ref, inner_ref = loaded[:3]
    experts = lax.axis_size("ep")
    lanes, seqs = share_ref.shape[1], share_ref.shape[0]
    inner = inner_ref[...]
    weight = group_ref[...] * inner / jnp.sum(inner, axis=0, keepdims=True)
    place = lax.broadcasted_iota(jnp.int32, (lanes, seqs), 0)
    owner = jnp.where(place >= experts, place - experts, place)
    share = jnp.zeros((lanes, seqs), wide)
    for k in range(ids_ref.shape[0]):
        share = share + jnp.where(owner == ids_ref[k : k + 1, :], weight[k : k + 1, :], 0.0)
    high = share.astype(narrow).astype(wide)
    packed = jnp.where(place < experts, high, jnp.where(place < 2 * experts, share - high, 0.0))
    share_ref[...] = packed.T.astype(narrow)
    for copy in copies[3:]:
        copy.wait()


def project_kernel(chips, gain_ref, *refs):
    blocks, (own_ref, other_ref), outs = refs[:chips], refs[chips : chips + 2], refs[chips + 2 :]
    me = lax.axis_index("ep")
    first = me % 2 == 0
    feats = own_ref.shape[0]
    pair_gain = gain_ref[:, pl.ds(pl.multiple_of(me // 2 * 2 * feats, lane_tile), 2 * feats)]
    rows = jnp.concatenate([block[...] for block in blocks], axis=0).astype(wide) * pair_gain
    low, high = rows[:, :feats], rows[:, feats:]
    mine = jnp.where(first, low, high).astype(narrow)
    others = jnp.where(first, high, low).astype(narrow)
    product = jnp.dot(mine, own_ref[...], preferred_element_type=wide)
    product = product + jnp.dot(others, other_ref[...], preferred_element_type=wide)
    seqs = outs[0].shape[0]
    for k, out in enumerate(outs):
        out[...] = product[k * seqs : (k + 1) * seqs].astype(out.dtype)


def recurrent_kernel(chips, cuts, base_ref, *refs):
    arrived, refs = refs[: chips - 1], refs[chips - 1 :]
    scale_ref, rate_ref, state_ref, gain_ref, output_ref, part_ref, read_ref = refs
    query_cols, value_cols = cuts
    seqs, heads, key_width, value_width = state_ref.shape
    total = base_ref[...]
    for block in arrived:
        total = total + block[...].astype(wide)
    total = total * scale_ref[:, :1]
    rounded = total.astype(narrow).astype(wide)
    pre = total[:, 2 * query_cols : 3 * query_cols]
    log_gate = jnp.minimum(pre, 0.0) - jnp.log1p(jnp.exp(-jnp.abs(pre)))
    decay = jnp.exp(log_gate * rate_ref[...])
    query = rounded[:, :query_cols] * key_width ** (-0.5)
    keys = rounded[:, query_cols : 2 * query_cols]
    turned = (query * decay).T
    out = None
    for h in range(heads):
        span = slice(h * key_width, (h + 1) * key_width)
        at = 3 * query_cols + h * value_width
        values = rounded[:, at : at + value_width]
        gates = rounded[:, at + value_cols : at + value_cols + value_width]
        for s in range(seqs):
            column = turned[span, s : s + 1]
            read_ref[s : s + 1, :] = jnp.sum(column * state_ref[s, h], axis=0, keepdims=True)
        match = jnp.sum(query[:, span] * keys[:, span], axis=1, keepdims=True)
        readout = read_ref[...] + match * values
        gated = (readout * inverse_rms(readout) * gain_ref[...] * silu(gates)).astype(narrow)
        rows = slice(h * value_width, (h + 1) * value_width)
        part = jnp.dot(gated, output_ref[rows, :], preferred_element_type=wide)
        out = part if out is None else out + part
    part_ref[...] = out.astype(narrow)


def mix_kernel(others, tokens_ref, part_ref, *refs):
    arrived, (gain_ref, share_ref, send_ref, own_ref) = refs[:others], refs[others:]
    width = tokens_ref.shape[1]
    attention = part_ref[...].astype(wide)
    for block in arrived:
        attention = attention + block[...].astype(wide)
    mixed = (tokens_ref[...].astype(wide) + attention).astype(narrow).astype(wide)
    send_ref[:, :width] = (mixed * inverse_rms(mixed) * gain_ref[...]).astype(narrow)
    send_ref[:, width:] = share_ref[...]
    cols = own_ref.shape[1]
    head = lax.axis_index("tp")
    attention = jnp.zeros(own_ref.shape, wide)
    at = pl.ds(pl.multiple_of(head * cols, lane_tile), cols)
    for block in (part_ref, *arrived):
        attention = attention + block[:, at].astype(wide)
    own_ref[...] = (tokens_ref[:, at].astype(wide) + attention).astype(narrow).astype(wide)


def expert_kernel(count, *refs):
    blocks, weights, outs = refs[:count], refs[count : count + 6], refs[count + 6 :]
    width = weights[0].shape[1]
    rows = jnp.concatenate([block[:, :width] for block in blocks], axis=0)
    share = jnp.concatenate([block[:, width:] for block in blocks], axis=0).astype(wide)
    me, experts = lax.axis_index("ep"), lax.axis_size("ep")
    head = lax.axis_index("tp")
    place = lax.broadcasted_iota(jnp.int32, share.shape, 1)
    hiddens, factors = [], []
    for n in range(2):
        gate_ref, up_ref = weights[3 * n], weights[3 * n + 1]
        chosen = (place == me ^ n) | (place == (me ^ n) + experts)
        factors.append(jnp.sum(jnp.where(chosen, share, 0.0), axis=1, keepdims=True))
        gate = jnp.dot(rows, gate_ref[0], preferred_element_type=wide)
        upper = jnp.dot(rows, up_ref[0], preferred_element_type=wide)
        hiddens.append((silu(gate) * upper).astype(narrow))
    cols = outs[0].shape[1]
    for k, out in enumerate(outs):
        at = pl.ds(pl.multiple_of((head ^ k) * cols, lane_tile), cols)
        total = None
        for n in range(2):
            down_ref = weights[3 * n + 2]
            part = jnp.dot(hiddens[n], down_ref[0, :, at], preferred_element_type=wide) * factors[n]
            total = part if total is None else total + part
        out[...] = total.astype(out.dtype)


def on_device(
    tokens,
    norm_gain,
    w_query,
    w_key,
    w_decay,
    w_value,
    w_outgate,
    decay_rate,
    state,
    head_gain,
    w_output,
    moe_gain,
    expert_ids,
    group_prob,
    inner_prob,
    w_gate,
    w_up,
    w_down,
):
    seqs, width = tokens.shape
    ep_count, tp_count = lax.axis_size("ep"), lax.axis_size("tp")
    chips = ep_count // 2
    half = chips * seqs
    _, _, value_width = state.shape[1:]
    feats = w_query.shape[0]
    query_cols, value_cols = w_query.shape[1], w_value.shape[1]
    proj_cols = 3 * query_cols + 2 * value_cols
    cols = width // tp_count
    lanes = -(-2 * ep_count // lane_tile) * lane_tile
    mib = 1 << 20

    weights = (w_query, w_key, w_decay, w_value, w_outgate)
    *pair_cols, tokens_near, joined = load_call(
        functools.partial(spread_kernel, len(weights)),
        (tokens, *weights),
        [like((seqs, 2 * feats), narrow)] * chips
        + [like(tokens.shape, narrow), like((feats, proj_cols), narrow)],
        chips + 1 + len(weights),
    )
    blocks = [pair_cols[0], *swap_chips(pair_cols)]
    joined_other = swap_core(joined)
    side_args = (
        expert_ids.T,
        group_prob[None, :],
        inner_prob.T,
        norm_gain[None, :],
        decay_rate[None, :],
        head_gain[None, :],
        moe_gain[None, :],
        w_output,
        state,
    )
    loaded = load_call(
        functools.partial(side_kernel, len(side_args)),
        side_args,
        [like(a.shape, a.dtype) for a in side_args]
        + [like((seqs, lane_tile), wide), like((seqs, lanes), narrow)],
        len(side_args),
        near=(tokens_near,),
    )
    gain, rate, read_gain, mix_gain, output_near, state_near, scale, share = loaded[3:]
    base, *sums = call(
        functools.partial(project_kernel, chips),
        [like((seqs, proj_cols), wide)] + [like((seqs, proj_cols), narrow)] * (chips - 1),
        (gain, *blocks, joined, joined_other),
        8 * mib,
    )
    arrived = swap_chips([base, *sums])
    expert_weights = (w_gate, w_up, w_down)
    expert_weights = load_call(
        functools.partial(load_kernel, 3),
        expert_weights,
        [like(a.shape, a.dtype) for a in expert_weights],
        3,
    )
    other_weights = []
    for weight in expert_weights:
        other_weights.append(swap_core(weight))
    (part,) = pl.pallas_call(
        functools.partial(recurrent_kernel, chips, (query_cols, value_cols)),
        out_shape=(like((seqs, width), narrow),),
        in_specs=[pl.BlockSpec(memory_space=pltpu.VMEM)] * (chips + 5),
        out_specs=(pl.BlockSpec(memory_space=pltpu.VMEM),),
        scratch_shapes=[pltpu.VMEM((seqs, value_width), wide)],
        compiler_params=pltpu.CompilerParams(vmem_limit_bytes=8 * mib),
        cost_estimate=pl.CostEstimate(flops=1 << 20, bytes_accessed=4 << 20, transcendentals=0),
        name="recurrent",
    )(base, *arrived, scale, rate, state_near, read_gain, output_near)
    parts = swap_heads([part] * tp_count, 0)
    sending, mixed_own = call(
        functools.partial(mix_kernel, tp_count - 1),
        [like((seqs, width + lanes), narrow), like((seqs, cols), wide)],
        (tokens_near, part, *parts, mix_gain, share),
        4 * mib,
    )
    rows = [sending, *swap_chips([sending] * chips)]
    head_sum, *pieces = call(
        functools.partial(expert_kernel, chips),
        [like((half, cols), wide)] + [like((half, cols), narrow)] * (tp_count - 1),
        (*rows, *expert_weights, *other_weights),
        24 * mib,
    )
    for block in swap_heads([head_sum, *pieces], 0):
        head_sum = head_sum + block.astype(wide)
    head_narrow = head_sum.astype(narrow)
    moe_sum = head_sum[:seqs]
    for block in swap_chips([head_narrow[k * seqs : (k + 1) * seqs] for k in range(chips)]):
        moe_sum = moe_sum + block.astype(wide)
    return (mixed_own + moe_sum).astype(narrow)


def solution(mesh):
    placed = (
        P("ep", None),
        P(),
        P("ep", "tp"),
        P("ep", "tp"),
        P("ep", "tp"),
        P("ep", "tp"),
        P("ep", "tp"),
        P("tp"),
        P("ep", "tp", None, None),
        P(),
        P("tp", None),
        P(),
        P("ep", None),
        P("ep"),
        P("ep", None),
        P("ep", None, "tp"),
        P("ep", None, "tp"),
        P("ep", "tp", None),
    )

    return jax.shard_map(
        on_device, mesh=mesh, in_specs=placed, out_specs=P("ep", "tp"), check_vma=False
    )
```

```python
import functools

import jax
import jax.numpy as jnp
from jax import lax
from jax.experimental import pallas as pl
from jax.experimental.pallas import tpu as pltpu
from jax.sharding import PartitionSpec as P


epsilon = 1e-05
wide = jnp.float32
narrow = jnp.bfloat16
lane_tile = 128


def inverse_rms(values):
    return lax.rsqrt(jnp.mean(values * values, axis=-1, keepdims=True) + epsilon)


def silu(values):
    return values / (1.0 + jnp.exp(-values))


def swap_core(block):
    count = lax.axis_size("ep")
    return lax.ppermute(block, "ep", [(i, i ^ 1) for i in range(count)])


def swap_chips(blocks):
    count = lax.axis_size("ep")
    got = {}
    for k in range(len(blocks) - 1, 0, -1):
        got[k] = lax.ppermute(blocks[k], "ep", [(i, i ^ (2 * k + 1)) for i in range(count)])
    return [got[k] for k in range(1, len(blocks))]


def swap_heads(blocks, other_core):
    ep_count, count = lax.axis_size("ep"), lax.axis_size("tp")
    got = {}
    for k in range(len(blocks) - 1, 0, -1):
        pairs = [
            (e * count + t, (e ^ other_core) * count + (t ^ k))
            for e in range(ep_count)
            for t in range(count)
        ]
        got[k] = lax.ppermute(blocks[k], ("ep", "tp"), pairs)
    return [got[k] for k in range(1, len(blocks))]


def call(kernel, outs, args, limit, flops=0):
    nbytes = sum(a.size * a.dtype.itemsize for a in args)
    nbytes += sum(o.size * o.dtype.itemsize for o in outs)
    return pl.pallas_call(
        kernel,
        out_shape=tuple(outs),
        in_specs=[pl.BlockSpec(memory_space=pltpu.VMEM)] * len(args),
        out_specs=tuple(pl.BlockSpec(memory_space=pltpu.VMEM) for _ in outs),
        compiler_params=pltpu.CompilerParams(vmem_limit_bytes=limit),
        cost_estimate=pl.CostEstimate(flops=flops, bytes_accessed=nbytes, transcendentals=0),
    )(*args)


def load_call(kernel, args, outs, copies, near=()):
    return pl.pallas_call(
        kernel,
        out_shape=tuple(outs),
        in_specs=[pl.BlockSpec(memory_space=pltpu.VMEM)] * len(near)
        + [pl.BlockSpec(memory_space=pltpu.HBM)] * len(args),
        out_specs=tuple(pl.BlockSpec(memory_space=pltpu.VMEM) for _ in outs),
        scratch_shapes=[pltpu.SemaphoreType.DMA((copies,))],
        compiler_params=pltpu.CompilerParams(vmem_limit_bytes=2 << 20),
        cost_estimate=pl.CostEstimate(flops=1 << 22, bytes_accessed=1 << 22, transcendentals=0),
    )(*near, *[pltpu.with_memory_space_constraint(a, pltpu.HBM) for a in args])


def like(shape, dtype):
    return jax.ShapeDtypeStruct(shape, dtype)


def load(pairs, sems):
    copies = [pltpu.make_async_copy(src, dst, sems.at[n]) for n, (src, dst) in enumerate(pairs)]
    for copy in copies:
        copy.start()
    return copies


def load_kernel(count, *refs):
    for copy in load(list(zip(refs[:count], refs[count : 2 * count])), refs[-1]):
        copy.wait()


def spread_kernel(tokens_ref, *refs):
    *block_refs, near_ref, sems = refs
    chip = lax.axis_index("ep") // 2
    cols = block_refs[0].shape[1]
    pairs = []
    for k in range(len(block_refs) - 1, -1, -1):
        at = pl.ds(pl.multiple_of((chip ^ k) * cols, lane_tile), cols)
        pairs.append((tokens_ref.at[:, at], block_refs[k]))
    pairs.append((tokens_ref, near_ref))
    for copy in load(pairs, sems):
        copy.wait()


def join_kernel(*refs):
    *weight_refs, joined_ref, sems = refs
    pairs, at = [], 0
    for weight in weight_refs:
        pairs.append((weight, joined_ref.at[:, at : at + weight.shape[1]]))
        at += weight.shape[1]
    for copy in load(pairs, sems):
        copy.wait()


def side_kernel(count, *refs):
    tokens_ref, refs = refs[0], refs[1:]
    loaded = refs[count : 2 * count]
    scale_ref, share_ref, sems = refs[2 * count :]
    copies = load(list(zip(refs[:count], loaded)), sems)
    scale_ref[...] = jnp.broadcast_to(inverse_rms(tokens_ref[...].astype(wide)), scale_ref.shape)
    for copy in copies[:3]:
        copy.wait()
    ids_ref, group_ref, inner_ref = loaded[:3]
    experts = lax.axis_size("ep")
    lanes, seqs = share_ref.shape[1], share_ref.shape[0]
    inner = inner_ref[...]
    weight = group_ref[...] * inner / jnp.sum(inner, axis=0, keepdims=True)
    place = lax.broadcasted_iota(jnp.int32, (lanes, seqs), 0)
    owner = jnp.where(place >= experts, place - experts, place)
    share = jnp.zeros((lanes, seqs), wide)
    for k in range(ids_ref.shape[0]):
        share = share + jnp.where(owner == ids_ref[k : k + 1, :], weight[k : k + 1, :], 0.0)
    high = share.astype(narrow).astype(wide)
    packed = jnp.where(place < experts, high, jnp.where(place < 2 * experts, share - high, 0.0))
    share_ref[...] = packed.T.astype(narrow)
    for copy in copies[3:]:
        copy.wait()


def project_kernel(chips, gain_ref, *refs):
    blocks, (own_ref, other_ref), outs = refs[:chips], refs[chips : chips + 2], refs[chips + 2 :]
    me = lax.axis_index("ep")
    first = me % 2 == 0
    feats = own_ref.shape[0]
    pair_gain = gain_ref[:, pl.ds(pl.multiple_of(me // 2 * 2 * feats, lane_tile), 2 * feats)]
    rows = jnp.concatenate([block[...] for block in blocks], axis=0).astype(wide) * pair_gain
    low, high = rows[:, :feats], rows[:, feats:]
    mine = jnp.where(first, low, high).astype(narrow)
    others = jnp.where(first, high, low).astype(narrow)
    product = jnp.dot(mine, own_ref[...], preferred_element_type=wide)
    product = product + jnp.dot(others, other_ref[...], preferred_element_type=wide)
    seqs = outs[0].shape[0]
    for k, out in enumerate(outs):
        out[...] = product[k * seqs : (k + 1) * seqs].astype(out.dtype)


def recurrent_kernel(chips, cuts, base_ref, *refs):
    arrived, refs = refs[: chips - 1], refs[chips - 1 :]
    scale_ref, rate_ref, state_ref, gain_ref, output_ref, part_ref, read_ref = refs
    query_cols, value_cols = cuts
    seqs, heads, key_width, value_width = state_ref.shape
    total = base_ref[...]
    for block in arrived:
        total = total + block[...].astype(wide)
    total = total * scale_ref[:, :1]
    rounded = total.astype(narrow).astype(wide)
    pre = total[:, 2 * query_cols : 3 * query_cols]
    log_gate = jnp.minimum(pre, 0.0) - jnp.log1p(jnp.exp(-jnp.abs(pre)))
    decay = jnp.exp(log_gate * rate_ref[...])
    query = rounded[:, :query_cols] * key_width ** (-0.5)
    keys = rounded[:, query_cols : 2 * query_cols]
    turned = (query * decay).T
    out = None
    for h in range(heads):
        span = slice(h * key_width, (h + 1) * key_width)
        at = 3 * query_cols + h * value_width
        values = rounded[:, at : at + value_width]
        gates = rounded[:, at + value_cols : at + value_cols + value_width]
        for s in range(seqs):
            column = turned[span, s : s + 1]
            read_ref[s : s + 1, :] = jnp.sum(column * state_ref[s, h], axis=0, keepdims=True)
        match = jnp.sum(query[:, span] * keys[:, span], axis=1, keepdims=True)
        readout = read_ref[...] + match * values
        gated = (readout * inverse_rms(readout) * gain_ref[...] * silu(gates)).astype(narrow)
        rows = slice(h * value_width, (h + 1) * value_width)
        part = jnp.dot(gated, output_ref[rows, :], preferred_element_type=wide)
        out = part if out is None else out + part
    part_ref[...] = out.astype(narrow)


def mix_kernel(others, tokens_ref, part_ref, *refs):
    arrived, (gain_ref, share_ref, send_ref, own_ref) = refs[:others], refs[others:]
    width = tokens_ref.shape[1]
    attention = part_ref[...].astype(wide)
    for block in arrived:
        attention = attention + block[...].astype(wide)
    mixed = (tokens_ref[...].astype(wide) + attention).astype(narrow).astype(wide)
    send_ref[:, :width] = (mixed * inverse_rms(mixed) * gain_ref[...]).astype(narrow)
    send_ref[:, width:] = share_ref[...]
    cols = own_ref.shape[1]
    head = lax.axis_index("tp")
    attention = jnp.zeros(own_ref.shape, wide)
    at = pl.ds(pl.multiple_of(head * cols, lane_tile), cols)
    for block in (part_ref, *arrived):
        attention = attention + block[:, at].astype(wide)
    own_ref[...] = (tokens_ref[:, at].astype(wide) + attention).astype(narrow).astype(wide)


def expert_kernel(count, *refs):
    blocks, weights, outs = refs[:count], refs[count : count + 6], refs[count + 6 :]
    width = weights[0].shape[1]
    rows = jnp.concatenate([block[:, :width] for block in blocks], axis=0)
    share = jnp.concatenate([block[:, width:] for block in blocks], axis=0).astype(wide)
    me, experts = lax.axis_index("ep"), lax.axis_size("ep")
    head = lax.axis_index("tp")
    place = lax.broadcasted_iota(jnp.int32, share.shape, 1)
    *pieces, first_hidden, second_hidden, factor_ref = outs
    hiddens, factors = [], []
    for n, hidden_ref in enumerate((first_hidden, second_hidden)):
        gate_ref, up_ref = weights[3 * n], weights[3 * n + 1]
        chosen = (place == me ^ n) | (place == (me ^ n) + experts)
        factors.append(jnp.sum(jnp.where(chosen, share, 0.0), axis=1, keepdims=True))
        gate = jnp.dot(rows, gate_ref[0], preferred_element_type=wide)
        upper = jnp.dot(rows, up_ref[0], preferred_element_type=wide)
        hiddens.append((silu(gate) * upper).astype(narrow))
        hidden_ref[...] = hiddens[n]
        factor_ref[:, n : n + 1] = factors[n]
    cols = pieces[0].shape[1]
    for k, out in enumerate(pieces):
        at = pl.ds(pl.multiple_of((head ^ (k + 1)) * cols, lane_tile), cols)
        out[...] = weighted(hiddens, factors, (weights[2], weights[5]), at).astype(out.dtype)


def weighted(hiddens, factors, downs, at):
    parts = [
        jnp.dot(hidden, down[0, :, at], preferred_element_type=wide) * factor
        for hidden, factor, down in zip(hiddens, factors, downs)
    ]
    return parts[0] + parts[1]


def near_kernel(first_ref, second_ref, factor_ref, down_ref, other_down_ref, out_ref):
    cols = out_ref.shape[1]
    at = pl.ds(pl.multiple_of(lax.axis_index("tp") * cols, lane_tile), cols)
    factors = factor_ref[:, 0:1], factor_ref[:, 1:2]
    hiddens = first_ref[...], second_ref[...]
    out_ref[...] = weighted(hiddens, factors, (down_ref, other_down_ref), at)


def on_device(
    tokens,
    norm_gain,
    w_query,
    w_key,
    w_decay,
    w_value,
    w_outgate,
    decay_rate,
    state,
    head_gain,
    w_output,
    moe_gain,
    expert_ids,
    group_prob,
    inner_prob,
    w_gate,
    w_up,
    w_down,
):
    seqs, width = tokens.shape
    ep_count, tp_count = lax.axis_size("ep"), lax.axis_size("tp")
    chips = ep_count // 2
    half = chips * seqs
    _, _, value_width = state.shape[1:]
    feats = w_query.shape[0]
    query_cols, value_cols = w_query.shape[1], w_value.shape[1]
    proj_cols = 3 * query_cols + 2 * value_cols
    cols = width // tp_count
    lanes = -(-2 * ep_count // lane_tile) * lane_tile
    mib = 1 << 20

    weights = (w_query, w_key, w_decay, w_value, w_outgate)
    *pair_cols, tokens_near = load_call(
        spread_kernel,
        (tokens,),
        [like((seqs, 2 * feats), narrow)] * chips + [like(tokens.shape, narrow)],
        chips + 1,
    )
    (joined,) = load_call(join_kernel, weights, [like((feats, proj_cols), narrow)], len(weights))
    blocks = [pair_cols[0], *swap_chips(pair_cols)]
    joined_other = swap_core(joined)
    side_args = (
        expert_ids.T,
        group_prob[None, :],
        inner_prob.T,
        norm_gain[None, :],
        decay_rate[None, :],
        head_gain[None, :],
        moe_gain[None, :],
    )
    loaded = load_call(
        functools.partial(side_kernel, len(side_args)),
        side_args,
        [like(a.shape, a.dtype) for a in side_args]
        + [like((seqs, lane_tile), wide), like((seqs, lanes), narrow)],
        len(side_args),
        near=(tokens_near,),
    )
    gain, rate, read_gain, mix_gain, scale, share = loaded[3:]
    base, *sums = call(
        functools.partial(project_kernel, chips),
        [like((seqs, proj_cols), wide)] + [like((seqs, proj_cols), narrow)] * (chips - 1),
        (gain, *blocks, joined, joined_other),
        8 * mib,
    )
    arrived = swap_chips([base, *sums])
    output_near, state_near = load_call(
        functools.partial(load_kernel, 2),
        (w_output, state),
        [like(a.shape, a.dtype) for a in (w_output, state)],
        2,
    )
    expert_weights, other_weights = (w_gate, w_up, w_down), []
    for weight in expert_weights:
        other_weights.append(swap_core(weight))
    (part,) = pl.pallas_call(
        functools.partial(recurrent_kernel, chips, (query_cols, value_cols)),
        out_shape=(like((seqs, width), narrow),),
        in_specs=[pl.BlockSpec(memory_space=pltpu.VMEM)] * (chips + 5),
        out_specs=(pl.BlockSpec(memory_space=pltpu.VMEM),),
        scratch_shapes=[pltpu.VMEM((seqs, value_width), wide)],
        compiler_params=pltpu.CompilerParams(vmem_limit_bytes=8 * mib),
        cost_estimate=pl.CostEstimate(flops=1 << 20, bytes_accessed=4 << 20, transcendentals=0),
        name="recurrent",
    )(base, *arrived, scale, rate, state_near, read_gain, output_near)
    parts = swap_heads([part] * tp_count, 0)
    sending, mixed_own = call(
        functools.partial(mix_kernel, tp_count - 1),
        [like((seqs, width + lanes), narrow), like((seqs, cols), wide)],
        (tokens_near, part, *parts, mix_gain, share),
        4 * mib,
    )
    rows = [sending, *swap_chips([sending] * chips)]
    expert_weights = load_call(
        functools.partial(load_kernel, 3),
        expert_weights,
        [like(a.shape, a.dtype) for a in expert_weights],
        3,
    )
    hidden_cols = w_gate.shape[2]
    *pieces, first_hidden, second_hidden, factor = call(
        functools.partial(expert_kernel, chips),
        [like((half, cols), narrow)] * (tp_count - 1)
        + [like((half, hidden_cols), narrow)] * 2
        + [like((half, lane_tile), wide)],
        (*rows, *expert_weights, *other_weights),
        24 * mib,
    )
    arrived = swap_heads([None, *pieces], 0)
    (head_sum,) = call(
        near_kernel,
        [like((half, cols), wide)],
        (first_hidden, second_hidden, factor, expert_weights[2], other_weights[2]),
        16 * mib,
    )
    for block in arrived:
        head_sum = head_sum + block.astype(wide)
    head_narrow = head_sum.astype(narrow)
    moe_sum = head_sum[:seqs]
    for block in swap_chips([head_narrow[k * seqs : (k + 1) * seqs] for k in range(chips)]):
        moe_sum = moe_sum + block.astype(wide)
    return (mixed_own + moe_sum).astype(narrow)


def solution(mesh):
    placed = (
        P("ep", None),
        P(),
        P("ep", "tp"),
        P("ep", "tp"),
        P("ep", "tp"),
        P("ep", "tp"),
        P("ep", "tp"),
        P("tp"),
        P("ep", "tp", None, None),
        P(),
        P("tp", None),
        P(),
        P("ep", None),
        P("ep"),
        P("ep", None),
        P("ep", None, "tp"),
        P("ep", None, "tp"),
        P("ep", "tp", None),
    )

    return jax.shard_map(
        on_device, mesh=mesh, in_specs=placed, out_specs=P("ep", "tp"), check_vma=False
    )
```

```python
import functools

import jax
import jax.numpy as jnp
from jax import lax
from jax.experimental import pallas as pl
from jax.experimental.pallas import tpu as pltpu
from jax.sharding import PartitionSpec as P


epsilon = 1e-05
wide = jnp.float32
narrow = jnp.bfloat16
lane_tile = 128


def inverse_rms(values):
    return lax.rsqrt(jnp.mean(values * values, axis=-1, keepdims=True) + epsilon)


def silu(values):
    return values / (1.0 + jnp.exp(-values))


def swap_core(block):
    count = lax.axis_size("ep")
    return lax.ppermute(block, "ep", [(i, i ^ 1) for i in range(count)])


def exchange(blocks, axis, sender):
    ep_count, tp_count = lax.axis_size("ep"), lax.axis_size("tp")
    got = {}
    for k in range(len(blocks) - 1, -1, -1):
        pairs = []
        for e in range(sender, ep_count, 2):
            for t in range(tp_count):
                to_e, to_t = (e ^ (2 * k), t) if axis == "ep" else (e, t ^ k)
                pairs.append((e * tp_count + t, (to_e ^ 1) * tp_count + to_t))
                pairs.append(((e ^ 1) * tp_count + t, e * tp_count + t))
        got[k] = lax.ppermute(blocks[k], ("ep", "tp"), pairs)
    return [got[k] for k in range(len(blocks))]


def call(kernel, outs, args, limit, flops=0):
    nbytes = sum(a.size * a.dtype.itemsize for a in args)
    nbytes += sum(o.size * o.dtype.itemsize for o in outs)
    return pl.pallas_call(
        kernel,
        out_shape=tuple(outs),
        in_specs=[pl.BlockSpec(memory_space=pltpu.VMEM)] * len(args),
        out_specs=tuple(pl.BlockSpec(memory_space=pltpu.VMEM) for _ in outs),
        compiler_params=pltpu.CompilerParams(vmem_limit_bytes=limit),
        cost_estimate=pl.CostEstimate(flops=flops, bytes_accessed=nbytes, transcendentals=0),
    )(*args)


def load_call(kernel, args, outs, copies, near=()):
    return pl.pallas_call(
        kernel,
        out_shape=tuple(outs),
        in_specs=[pl.BlockSpec(memory_space=pltpu.VMEM)] * len(near)
        + [pl.BlockSpec(memory_space=pltpu.HBM)] * len(args),
        out_specs=tuple(pl.BlockSpec(memory_space=pltpu.VMEM) for _ in outs),
        scratch_shapes=[pltpu.SemaphoreType.DMA((copies,))],
        compiler_params=pltpu.CompilerParams(vmem_limit_bytes=2 << 20),
        cost_estimate=pl.CostEstimate(flops=1 << 22, bytes_accessed=1 << 22, transcendentals=0),
    )(*near, *[pltpu.with_memory_space_constraint(a, pltpu.HBM) for a in args])


def like(shape, dtype):
    return jax.ShapeDtypeStruct(shape, dtype)


def load(pairs, sems):
    copies = [pltpu.make_async_copy(src, dst, sems.at[n]) for n, (src, dst) in enumerate(pairs)]
    for copy in copies:
        copy.start()
    return copies


def load_kernel(count, *refs):
    for copy in load(list(zip(refs[:count], refs[count : 2 * count])), refs[-1]):
        copy.wait()


def spread_kernel(own_ref, other_ref, *block_refs):
    chip = lax.axis_index("ep") // 2
    seqs, cols = own_ref.shape[0], block_refs[0].shape[1]
    for k, out in enumerate(block_refs):
        at = pl.ds(pl.multiple_of((chip ^ k) * cols, lane_tile), cols)
        out[:seqs] = own_ref[:, at]
        out[seqs:] = other_ref[:, at]


def join_kernel(count, *refs):
    tokens_ref, *weight_refs, gain_ref = refs[:count]
    tokens_near_ref, joined_ref, near_ref, sems = refs[count:]
    pairs, at = [(tokens_ref, tokens_near_ref), (gain_ref, near_ref)], 0
    for weight in weight_refs:
        pairs.append((weight, joined_ref.at[:, at : at + weight.shape[1]]))
        at += weight.shape[1]
    for copy in load(pairs, sems):
        copy.wait()


def side_kernel(count, *refs):
    tokens_refs, refs = refs[:2], refs[2:]
    loaded = refs[count : 2 * count]
    scale_ref, share_ref, repeat_ref, sems = refs[2 * count :]
    spots, wides = repeat_ref.shape
    row = lax.broadcasted_iota(jnp.int32, (spots, wides), 0)
    col = lax.broadcasted_iota(jnp.int32, (spots, wides), 1)
    same = lax.rem(row, share_ref.shape[0]) == lax.shift_right_logical(col, 7)
    repeat_ref[...] = jnp.where(same, 1.0, 0.0).astype(narrow)
    copies = load(list(zip(refs[:count], loaded)), sems)
    seqs = share_ref.shape[0]
    for n, tokens_ref in enumerate(tokens_refs):
        inverse = inverse_rms(tokens_ref[...].astype(wide))
        scale_ref[n * seqs : (n + 1) * seqs] = jnp.broadcast_to(inverse, (seqs, scale_ref.shape[1]))
    for copy in copies[:3]:
        copy.wait()
    ids_ref, group_ref, inner_ref = loaded[:3]
    experts = lax.axis_size("ep")
    lanes = share_ref.shape[1]
    inner = inner_ref[...]
    weight = group_ref[...] * inner / jnp.sum(inner, axis=0, keepdims=True)
    place = lax.broadcasted_iota(jnp.int32, (lanes, seqs), 0)
    owner = jnp.where(place >= experts, place - experts, place)
    share = jnp.zeros((lanes, seqs), wide)
    for k in range(ids_ref.shape[0]):
        share = share + jnp.where(owner == ids_ref[k : k + 1, :], weight[k : k + 1, :], 0.0)
    high = share.astype(narrow).astype(wide)
    packed = jnp.where(place < experts, high, jnp.where(place < 2 * experts, share - high, 0.0))
    share_ref[...] = packed.T.astype(narrow)
    for copy in copies[3:]:
        copy.wait()


def project_kernel(chips, gain_ref, *refs):
    blocks, (own_ref, other_ref), outs = refs[:chips], refs[chips : chips + 2], refs[chips + 2 :]
    me = lax.axis_index("ep")
    first = me % 2 == 0
    feats = own_ref.shape[0]
    pair_gain = gain_ref[:, pl.ds(pl.multiple_of(me // 2 * 2 * feats, lane_tile), 2 * feats)]
    rows = jnp.concatenate([block[...] for block in blocks], axis=0).astype(wide) * pair_gain
    low, high = rows[:, :feats], rows[:, feats:]
    mine = jnp.where(first, low, high).astype(narrow)
    others = jnp.where(first, high, low).astype(narrow)
    product = jnp.dot(mine, own_ref[...], preferred_element_type=wide)
    product = product + jnp.dot(others, other_ref[...], preferred_element_type=wide)
    seqs = outs[0].shape[0]
    for k, out in enumerate(outs):
        out[...] = product[k * seqs : (k + 1) * seqs].astype(out.dtype)


def recurrent_kernel(chips, cuts, *refs):
    arrived, refs = refs[:chips], refs[chips:]
    scale_ref, repeat_ref, rate_ref, own_ref, other_ref, gain_ref, output_ref, part_ref, read_ref = refs
    query_cols, value_cols = cuts
    seqs, heads, key_width, value_width = own_ref.shape
    total = arrived[0][...].astype(wide)
    for block in arrived[1:]:
        total = total + block[...].astype(wide)
    total = total * scale_ref[:, :1]
    rounded = total.astype(narrow).astype(wide)
    pre = total[:, 2 * query_cols : 3 * query_cols]
    log_gate = jnp.minimum(pre, 0.0) - jnp.log1p(jnp.exp(-jnp.abs(pre)))
    decay = jnp.exp(log_gate * rate_ref[...])
    query = rounded[:, :query_cols] * key_width ** (-0.5)
    keys = rounded[:, query_cols : 2 * query_cols]
    driven = query * decay
    high = driven.astype(narrow).astype(wide)
    middle = (driven - high).astype(narrow).astype(wide)
    low = driven - high - middle
    turned = []
    for n in range(2):
        rows = slice(n * seqs, (n + 1) * seqs)
        parts = jnp.concatenate([high[rows], middle[rows], low[rows]], axis=0)
        turned.append(parts.T.astype(narrow))
    out = None
    for h in range(heads):
        span = slice(h * key_width, (h + 1) * key_width)
        at = 3 * query_cols + h * value_width
        values = rounded[:, at : at + value_width]
        gates = rounded[:, at + value_cols : at + value_cols + value_width]
        for n, state_ref in enumerate((own_ref, other_ref)):
            columns = jnp.dot(turned[n][span], repeat_ref[...], preferred_element_type=wide)
            for s in range(seqs):
                column = columns[:, s * lane_tile : (s + 1) * lane_tile]
                row = slice(n * seqs + s, n * seqs + s + 1)
                for lane in range(0, value_width, lane_tile):
                    product = column * state_ref[s, h, :, lane : lane + lane_tile]
                    read_ref[row, lane : lane + lane_tile] = jnp.sum(product, axis=0, keepdims=True)
        match = jnp.sum(query[:, span] * keys[:, span], axis=1, keepdims=True)
        readout = read_ref[...] + match * values
        gated = (readout * inverse_rms(readout) * gain_ref[...] * silu(gates)).astype(narrow)
        rows = slice(h * value_width, (h + 1) * value_width)
        part = jnp.dot(gated, output_ref[rows, :], preferred_element_type=wide)
        out = part if out is None else out + part
    part_ref[...] = out.astype(narrow)


def mix_kernel(count, *refs):
    arrived, refs = refs[:count], refs[count:]
    other_ref, own_ref, gain_ref, other_share_ref, own_share_ref, send_ref, mixed_ref = refs
    seqs, width = own_ref.shape
    tokens = jnp.concatenate([other_ref[...], own_ref[...]], axis=0).astype(wide)
    attention = arrived[0][...].astype(wide)
    for block in arrived[1:]:
        attention = attention + block[...].astype(wide)
    mixed = (tokens + attention).astype(narrow).astype(wide)
    send_ref[:, :width] = (mixed * inverse_rms(mixed) * gain_ref[...]).astype(narrow)
    send_ref[:seqs, width:] = other_share_ref[...]
    send_ref[seqs:, width:] = own_share_ref[...]
    cols = mixed_ref.shape[1]
    at = pl.ds(pl.multiple_of(lax.axis_index("tp") * cols, lane_tile), cols)
    attention = arrived[0][:, at].astype(wide)
    for block in arrived[1:]:
        attention = attention + block[:, at].astype(wide)
    tokens = jnp.concatenate([other_ref[:, at], own_ref[:, at]], axis=0).astype(wide)
    mixed_ref[...] = (tokens + attention).astype(narrow).astype(wide)


def expert_kernel(count, *refs):
    blocks, weights, outs = refs[:count], refs[count : count + 6], refs[count + 6 :]
    width = weights[0].shape[1]
    rows = jnp.concatenate([block[:, :width] for block in blocks], axis=0)
    share = jnp.concatenate([block[:, width:] for block in blocks], axis=0).astype(wide)
    me, experts = lax.axis_index("ep"), lax.axis_size("ep")
    head = lax.axis_index("tp")
    place = lax.broadcasted_iota(jnp.int32, share.shape, 1)
    hiddens, factors = [], []
    for n in range(2):
        gate_ref, up_ref = weights[3 * n], weights[3 * n + 1]
        chosen = (place == me ^ n) | (place == (me ^ n) + experts)
        factors.append(jnp.sum(jnp.where(chosen, share, 0.0), axis=1, keepdims=True))
        gate = jnp.dot(rows, gate_ref[0], preferred_element_type=wide)
        upper = jnp.dot(rows, up_ref[0], preferred_element_type=wide)
        hiddens.append((silu(gate) * upper).astype(narrow))
    cols = outs[0].shape[1]
    for k, out in enumerate(outs):
        at = pl.ds(pl.multiple_of((head ^ k) * cols, lane_tile), cols)
        parts = [
            jnp.dot(hidden, down[0, :, at], preferred_element_type=wide) * factor
            for hidden, down, factor in zip(hiddens, (weights[2], weights[5]), factors)
        ]
        out[...] = (parts[0] + parts[1]).astype(out.dtype)


def on_device(
    tokens,
    norm_gain,
    w_query,
    w_key,
    w_decay,
    w_value,
    w_outgate,
    decay_rate,
    state,
    head_gain,
    w_output,
    moe_gain,
    expert_ids,
    group_prob,
    inner_prob,
    w_gate,
    w_up,
    w_down,
):
    seqs, width = tokens.shape
    ep_count, tp_count = lax.axis_size("ep"), lax.axis_size("tp")
    chips = ep_count // 2
    pair = 2 * seqs
    _, _, value_width = state.shape[1:]
    feats = w_query.shape[0]
    query_cols, value_cols = w_query.shape[1], w_value.shape[1]
    proj_cols = 3 * query_cols + 2 * value_cols
    cols = width // tp_count
    lanes = -(-2 * ep_count // lane_tile) * lane_tile
    mib = 1 << 20

    tokens_other = swap_core(tokens)
    weights = (tokens, w_query, w_key, w_decay, w_value, w_outgate, norm_gain[None, :])
    tokens_near, joined, gain = load_call(
        functools.partial(join_kernel, len(weights)),
        weights,
        [
            like(tokens.shape, narrow),
            like((feats, proj_cols), narrow),
            like((1, width), wide),
        ],
        len(weights),
    )
    joined_other = swap_core(joined)
    expert_weights, other_weights = (w_gate, w_up, w_down), []
    for weight in expert_weights:
        other_weights.append(swap_core(weight))
    blocks = call(
        spread_kernel,
        [like((pair, 2 * feats), narrow)] * chips,
        (tokens_near, tokens_other),
        4 * mib,
    )
    blocks = exchange(blocks, "ep", 0)
    sums = call(
        functools.partial(project_kernel, chips),
        [like((pair, proj_cols), narrow)] * chips,
        (gain, *blocks, joined, joined_other),
        8 * mib,
    )
    sums = exchange(sums, "ep", 1)
    state_other = swap_core(state)
    side_args = (
        expert_ids.T,
        group_prob[None, :],
        inner_prob.T,
        decay_rate[None, :],
        head_gain[None, :],
        moe_gain[None, :],
        w_output,
        state,
    )
    loaded = load_call(
        functools.partial(side_kernel, len(side_args)),
        side_args,
        [like(a.shape, a.dtype) for a in side_args]
        + [
            like((pair, lane_tile), wide),
            like((seqs, lanes), narrow),
            like((3 * seqs, seqs * lane_tile), narrow),
        ],
        len(side_args),
        near=(tokens_near, tokens_other),
    )
    rate, read_gain, mix_gain, output_near, state_near, scale, share, repeat = loaded[3:]
    (part,) = pl.pallas_call(
        functools.partial(recurrent_kernel, chips, (query_cols, value_cols)),
        out_shape=(like((pair, width), narrow),),
        in_specs=[pl.BlockSpec(memory_space=pltpu.VMEM)] * (chips + 7),
        out_specs=(pl.BlockSpec(memory_space=pltpu.VMEM),),
        scratch_shapes=[pltpu.VMEM((pair, value_width), wide)],
        compiler_params=pltpu.CompilerParams(vmem_limit_bytes=8 * mib),
        cost_estimate=pl.CostEstimate(flops=1 << 21, bytes_accessed=8 << 20, transcendentals=0),
        name="recurrent",
    )(*sums, scale, repeat, rate, state_near, state_other, read_gain, output_near)
    parts = exchange([part] * tp_count, "tp", 0)
    share_other = swap_core(share)
    sending, mixed = call(
        functools.partial(mix_kernel, tp_count),
        [like((pair, width + lanes), narrow), like((pair, cols), wide)],
        (*parts, tokens_other, tokens_near, mix_gain, share_other, share),
        4 * mib,
    )
    rows = exchange([sending] * chips, "ep", 1)
    mixed = swap_core(mixed)
    expert_weights = load_call(
        functools.partial(load_kernel, 3),
        expert_weights,
        [like(a.shape, a.dtype) for a in expert_weights],
        3,
    )
    pieces = call(
        functools.partial(expert_kernel, chips),
        [like((chips * pair, cols), narrow)] * tp_count,
        (*rows, *expert_weights, *other_weights),
        24 * mib,
    )
    pieces = exchange(pieces, "tp", 0)
    head_sum = sum(piece.astype(wide) for piece in pieces).astype(narrow)
    backs = [head_sum[k * pair : (k + 1) * pair] for k in range(chips)]
    backs = exchange(backs, "ep", 1)
    result = (mixed + sum(back.astype(wide) for back in backs)).astype(narrow)
    arrived = swap_core(result[seqs:])
    return jnp.where(lax.axis_index("ep") % 2 == 0, result[:seqs], arrived)


def solution(mesh):
    placed = (
        P("ep", None),
        P(),
        P("ep", "tp"),
        P("ep", "tp"),
        P("ep", "tp"),
        P("ep", "tp"),
        P("ep", "tp"),
        P("tp"),
        P("ep", "tp", None, None),
        P(),
        P("tp", None),
        P(),
        P("ep", None),
        P("ep"),
        P("ep", None),
        P("ep", None, "tp"),
        P("ep", None, "tp"),
        P("ep", "tp", None),
    )

    return jax.shard_map(
        on_device, mesh=mesh, in_specs=placed, out_specs=P("ep", "tp"), check_vma=False
    )
```

```python
import functools

import jax
import jax.numpy as jnp
from jax import lax
from jax.experimental import pallas as pl
from jax.experimental.pallas import tpu as pltpu
from jax.sharding import PartitionSpec as P


epsilon = 1e-05
wide = jnp.float32
narrow = jnp.bfloat16
lane_tile = 128


def inverse_rms(values):
    return lax.rsqrt(jnp.mean(values * values, axis=-1, keepdims=True) + epsilon)


def silu(values):
    return values / (1.0 + jnp.exp(-values))


def swap_core(block):
    count = lax.axis_size("ep")
    return lax.ppermute(block, "ep", [(i, i ^ 1) for i in range(count)])


def exchange(blocks, axis, sender):
    ep_count, tp_count = lax.axis_size("ep"), lax.axis_size("tp")
    got = {}
    for k in range(len(blocks) - 1, -1, -1):
        pairs = []
        for e in range(sender, ep_count, 2):
            for t in range(tp_count):
                to_e, to_t = (e ^ (2 * k), t) if axis == "ep" else (e, t ^ k)
                pairs.append((e * tp_count + t, (to_e ^ 1) * tp_count + to_t))
                pairs.append(((e ^ 1) * tp_count + t, e * tp_count + t))
        got[k] = lax.ppermute(blocks[k], ("ep", "tp"), pairs)
    return [got[k] for k in range(len(blocks))]


def call(kernel, outs, args, limit, flops=0):
    nbytes = sum(a.size * a.dtype.itemsize for a in args)
    nbytes += sum(o.size * o.dtype.itemsize for o in outs)
    return pl.pallas_call(
        kernel,
        out_shape=tuple(outs),
        in_specs=[pl.BlockSpec(memory_space=pltpu.VMEM)] * len(args),
        out_specs=tuple(pl.BlockSpec(memory_space=pltpu.VMEM) for _ in outs),
        compiler_params=pltpu.CompilerParams(vmem_limit_bytes=limit),
        cost_estimate=pl.CostEstimate(flops=flops, bytes_accessed=nbytes, transcendentals=0),
    )(*args)


def only(core, kernel):
    def body(*refs):
        @pl.when(lax.axis_index("ep") % 2 == core)
        def _():
            kernel(*refs)

    return body


def load_call(kernel, args, outs, copies, near=()):
    return pl.pallas_call(
        kernel,
        out_shape=tuple(outs),
        in_specs=[pl.BlockSpec(memory_space=pltpu.VMEM)] * len(near)
        + [pl.BlockSpec(memory_space=pltpu.HBM)] * len(args),
        out_specs=tuple(pl.BlockSpec(memory_space=pltpu.VMEM) for _ in outs),
        scratch_shapes=[pltpu.SemaphoreType.DMA((copies,))],
        compiler_params=pltpu.CompilerParams(vmem_limit_bytes=2 << 20),
        cost_estimate=pl.CostEstimate(flops=1 << 22, bytes_accessed=1 << 22, transcendentals=0),
    )(*near, *[pltpu.with_memory_space_constraint(a, pltpu.HBM) for a in args])


def like(shape, dtype):
    return jax.ShapeDtypeStruct(shape, dtype)


def load(pairs, sems):
    copies = [pltpu.make_async_copy(src, dst, sems.at[n]) for n, (src, dst) in enumerate(pairs)]
    for copy in copies:
        copy.start()
    return copies


def load_kernel(count, *refs):
    for copy in load(list(zip(refs[:count], refs[count : 2 * count])), refs[-1]):
        copy.wait()


def spread_kernel(own_ref, other_ref, *block_refs):
    chip = lax.axis_index("ep") // 2
    seqs, cols = own_ref.shape[0], block_refs[0].shape[1]
    for k, out in enumerate(block_refs):
        at = pl.ds(pl.multiple_of((chip ^ k) * cols, lane_tile), cols)
        out[:seqs] = own_ref[:, at]
        out[seqs:] = other_ref[:, at]


def join_kernel(count, *refs):
    tokens_ref, *weight_refs, gain_ref = refs[:count]
    tokens_near_ref, joined_ref, near_ref, sems = refs[count:]
    pairs, at = [(tokens_ref, tokens_near_ref), (gain_ref, near_ref)], 0
    for weight in weight_refs:
        pairs.append((weight, joined_ref.at[:, at : at + weight.shape[1]]))
        at += weight.shape[1]
    for copy in load(pairs, sems):
        copy.wait()


def side_kernel(count, *refs):
    tokens_refs, refs = refs[:2], refs[2:]
    loaded = refs[count : 2 * count]
    scale_ref, share_ref, repeat_ref, sems = refs[2 * count :]
    spots, wides = repeat_ref.shape
    row = lax.broadcasted_iota(jnp.int32, (spots, wides), 0)
    col = lax.broadcasted_iota(jnp.int32, (spots, wides), 1)
    same = lax.rem(row, share_ref.shape[0]) == lax.shift_right_logical(col, 7)
    repeat_ref[...] = jnp.where(same, 1.0, 0.0).astype(narrow)
    copies = load(list(zip(refs[:count], loaded)), sems)
    seqs = share_ref.shape[0]
    for n, tokens_ref in enumerate(tokens_refs):
        inverse = inverse_rms(tokens_ref[...].astype(wide))
        scale_ref[n * seqs : (n + 1) * seqs] = jnp.broadcast_to(inverse, (seqs, scale_ref.shape[1]))
    for copy in copies[:3]:
        copy.wait()
    ids_ref, group_ref, inner_ref = loaded[:3]
    experts = lax.axis_size("ep")
    lanes = share_ref.shape[1]
    inner = inner_ref[...]
    weight = group_ref[...] * inner / jnp.sum(inner, axis=0, keepdims=True)
    place = lax.broadcasted_iota(jnp.int32, (lanes, seqs), 0)
    owner = jnp.where(place >= experts, place - experts, place)
    share = jnp.zeros((lanes, seqs), wide)
    for k in range(ids_ref.shape[0]):
        share = share + jnp.where(owner == ids_ref[k : k + 1, :], weight[k : k + 1, :], 0.0)
    high = share.astype(narrow).astype(wide)
    packed = jnp.where(place < experts, high, jnp.where(place < 2 * experts, share - high, 0.0))
    share_ref[...] = packed.T.astype(narrow)
    for copy in copies[3:]:
        copy.wait()


def project_kernel(chips, gain_ref, *refs):
    blocks, (own_ref, other_ref), outs = refs[:chips], refs[chips : chips + 2], refs[chips + 2 :]
    me = lax.axis_index("ep")
    first = me % 2 == 0
    feats = own_ref.shape[0]
    pair_gain = gain_ref[:, pl.ds(pl.multiple_of(me // 2 * 2 * feats, lane_tile), 2 * feats)]
    rows = jnp.concatenate([block[...] for block in blocks], axis=0).astype(wide) * pair_gain
    low, high = rows[:, :feats], rows[:, feats:]
    mine = jnp.where(first, low, high).astype(narrow)
    others = jnp.where(first, high, low).astype(narrow)
    product = jnp.dot(mine, own_ref[...], preferred_element_type=wide)
    product = product + jnp.dot(others, other_ref[...], preferred_element_type=wide)
    seqs = outs[0].shape[0]
    for k, out in enumerate(outs):
        out[...] = product[k * seqs : (k + 1) * seqs].astype(out.dtype)


def recurrent_kernel(chips, cuts, *refs):
    arrived, refs = refs[:chips], refs[chips:]
    scale_ref, repeat_ref, rate_ref, own_ref, other_ref, gain_ref, output_ref, part_ref, read_ref = refs
    query_cols, value_cols = cuts
    seqs, heads, key_width, value_width = own_ref.shape
    total = arrived[0][...].astype(wide)
    for block in arrived[1:]:
        total = total + block[...].astype(wide)
    total = total * scale_ref[:, :1]
    rounded = total.astype(narrow).astype(wide)
    pre = total[:, 2 * query_cols : 3 * query_cols]
    log_gate = jnp.minimum(pre, 0.0) - jnp.log1p(jnp.exp(-jnp.abs(pre)))
    decay = jnp.exp(log_gate * rate_ref[...])
    query = rounded[:, :query_cols] * key_width ** (-0.5)
    keys = rounded[:, query_cols : 2 * query_cols]
    driven = query * decay
    high = driven.astype(narrow).astype(wide)
    middle = (driven - high).astype(narrow).astype(wide)
    low = driven - high - middle
    turned = []
    for n in range(2):
        rows = slice(n * seqs, (n + 1) * seqs)
        parts = jnp.concatenate([high[rows], middle[rows], low[rows]], axis=0)
        turned.append(parts.T.astype(narrow))
    out = None
    for h in range(heads):
        span = slice(h * key_width, (h + 1) * key_width)
        at = 3 * query_cols + h * value_width
        values = rounded[:, at : at + value_width]
        gates = rounded[:, at + value_cols : at + value_cols + value_width]
        for n, state_ref in enumerate((own_ref, other_ref)):
            columns = jnp.dot(turned[n][span], repeat_ref[...], preferred_element_type=wide)
            for s in range(seqs):
                column = columns[:, s * lane_tile : (s + 1) * lane_tile]
                row = slice(n * seqs + s, n * seqs + s + 1)
                for lane in range(0, value_width, lane_tile):
                    product = column * state_ref[s, h, :, lane : lane + lane_tile]
                    read_ref[row, lane : lane + lane_tile] = jnp.sum(product, axis=0, keepdims=True)
        match = jnp.sum(query[:, span] * keys[:, span], axis=1, keepdims=True)
        readout = read_ref[...] + match * values
        gated = (readout * inverse_rms(readout) * gain_ref[...] * silu(gates)).astype(narrow)
        rows = slice(h * value_width, (h + 1) * value_width)
        part = jnp.dot(gated, output_ref[rows, :], preferred_element_type=wide)
        out = part if out is None else out + part
    part_ref[...] = out.astype(narrow)


def mix_kernel(count, *refs):
    arrived, refs = refs[:count], refs[count:]
    other_ref, own_ref, gain_ref, other_share_ref, own_share_ref, send_ref, mixed_ref = refs
    seqs, width = own_ref.shape
    tokens = jnp.concatenate([other_ref[...], own_ref[...]], axis=0).astype(wide)
    attention = arrived[0][...].astype(wide)
    for block in arrived[1:]:
        attention = attention + block[...].astype(wide)
    mixed = (tokens + attention).astype(narrow).astype(wide)
    send_ref[:, :width] = (mixed * inverse_rms(mixed) * gain_ref[...]).astype(narrow)
    send_ref[:seqs, width:] = other_share_ref[...]
    send_ref[seqs:, width:] = own_share_ref[...]
    cols = mixed_ref.shape[1]
    at = pl.ds(pl.multiple_of(lax.axis_index("tp") * cols, lane_tile), cols)
    attention = arrived[0][:, at].astype(wide)
    for block in arrived[1:]:
        attention = attention + block[:, at].astype(wide)
    tokens = jnp.concatenate([other_ref[:, at], own_ref[:, at]], axis=0).astype(wide)
    mixed_ref[...] = (tokens + attention).astype(narrow).astype(wide)


def expert_kernel(count, *refs):
    blocks, weights, outs = refs[:count], refs[count : count + 6], refs[count + 6 :]
    width = weights[0].shape[1]
    rows = jnp.concatenate([block[:, :width] for block in blocks], axis=0)
    share = jnp.concatenate([block[:, width:] for block in blocks], axis=0).astype(wide)
    me, experts = lax.axis_index("ep"), lax.axis_size("ep")
    head = lax.axis_index("tp")
    place = lax.broadcasted_iota(jnp.int32, share.shape, 1)
    hiddens, factors = [], []
    for n in range(2):
        gate_ref, up_ref = weights[3 * n], weights[3 * n + 1]
        chosen = (place == me ^ n) | (place == (me ^ n) + experts)
        factors.append(jnp.sum(jnp.where(chosen, share, 0.0), axis=1, keepdims=True))
        gate = jnp.dot(rows, gate_ref[0], preferred_element_type=wide)
        upper = jnp.dot(rows, up_ref[0], preferred_element_type=wide)
        hiddens.append((silu(gate) * upper).astype(narrow))
    cols = outs[0].shape[1]
    for k, out in enumerate(outs):
        at = pl.ds(pl.multiple_of((head ^ k) * cols, lane_tile), cols)
        parts = [
            jnp.dot(hidden, down[0, :, at], preferred_element_type=wide) * factor
            for hidden, down, factor in zip(hiddens, (weights[2], weights[5]), factors)
        ]
        out[...] = (parts[0] + parts[1]).astype(out.dtype)


def on_device(
    tokens,
    norm_gain,
    w_query,
    w_key,
    w_decay,
    w_value,
    w_outgate,
    decay_rate,
    state,
    head_gain,
    w_output,
    moe_gain,
    expert_ids,
    group_prob,
    inner_prob,
    w_gate,
    w_up,
    w_down,
):
    seqs, width = tokens.shape
    ep_count, tp_count = lax.axis_size("ep"), lax.axis_size("tp")
    chips = ep_count // 2
    pair = 2 * seqs
    _, _, value_width = state.shape[1:]
    feats = w_query.shape[0]
    query_cols, value_cols = w_query.shape[1], w_value.shape[1]
    proj_cols = 3 * query_cols + 2 * value_cols
    cols = width // tp_count
    lanes = -(-2 * ep_count // lane_tile) * lane_tile
    mib = 1 << 20

    tokens_other = swap_core(tokens)
    weights = (tokens, w_query, w_key, w_decay, w_value, w_outgate, norm_gain[None, :])
    tokens_near, joined, gain = load_call(
        functools.partial(join_kernel, len(weights)),
        weights,
        [
            like(tokens.shape, narrow),
            like((feats, proj_cols), narrow),
            like((1, width), wide),
        ],
        len(weights),
    )
    joined_other = swap_core(joined)
    expert_weights, other_weights = (w_gate, w_up, w_down), []
    for weight in expert_weights:
        other_weights.append(swap_core(weight))
    blocks = call(
        spread_kernel,
        [like((pair, 2 * feats), narrow)] * chips,
        (tokens_near, tokens_other),
        4 * mib,
    )
    blocks = exchange(blocks, "ep", 0)
    sums = call(
        only(1, functools.partial(project_kernel, chips)),
        [like((pair, proj_cols), narrow)] * chips,
        (gain, *blocks, joined, joined_other),
        8 * mib,
    )
    sums = exchange(sums, "ep", 1)
    state_other = swap_core(state)
    side_args = (
        expert_ids.T,
        group_prob[None, :],
        inner_prob.T,
        decay_rate[None, :],
        head_gain[None, :],
        moe_gain[None, :],
        w_output,
        state,
    )
    loaded = load_call(
        functools.partial(side_kernel, len(side_args)),
        side_args,
        [like(a.shape, a.dtype) for a in side_args]
        + [
            like((pair, lane_tile), wide),
            like((seqs, lanes), narrow),
            like((3 * seqs, seqs * lane_tile), narrow),
        ],
        len(side_args),
        near=(tokens_near, tokens_other),
    )
    rate, read_gain, mix_gain, output_near, state_near, scale, share, repeat = loaded[3:]
    (part,) = pl.pallas_call(
        only(0, functools.partial(recurrent_kernel, chips, (query_cols, value_cols))),
        out_shape=(like((pair, width), narrow),),
        in_specs=[pl.BlockSpec(memory_space=pltpu.VMEM)] * (chips + 7),
        out_specs=(pl.BlockSpec(memory_space=pltpu.VMEM),),
        scratch_shapes=[pltpu.VMEM((pair, value_width), wide)],
        compiler_params=pltpu.CompilerParams(vmem_limit_bytes=8 * mib),
        cost_estimate=pl.CostEstimate(flops=1 << 21, bytes_accessed=8 << 20, transcendentals=0),
        name="recurrent",
    )(*sums, scale, repeat, rate, state_near, state_other, read_gain, output_near)
    parts = exchange([part] * tp_count, "tp", 0)
    share_other = swap_core(share)
    sending, mixed = call(
        only(1, functools.partial(mix_kernel, tp_count)),
        [like((pair, width + lanes), narrow), like((pair, cols), wide)],
        (*parts, tokens_other, tokens_near, mix_gain, share_other, share),
        4 * mib,
    )
    rows = exchange([sending] * chips, "ep", 1)
    mixed = swap_core(mixed)
    expert_weights = load_call(
        functools.partial(load_kernel, 3),
        expert_weights,
        [like(a.shape, a.dtype) for a in expert_weights],
        3,
    )
    pieces = call(
        only(0, functools.partial(expert_kernel, chips)),
        [like((chips * pair, cols), narrow)] * tp_count,
        (*rows, *expert_weights, *other_weights),
        24 * mib,
    )
    pieces = exchange(pieces, "tp", 0)
    head_sum = sum(piece.astype(wide) for piece in pieces).astype(narrow)
    backs = [head_sum[k * pair : (k + 1) * pair] for k in range(chips)]
    backs = exchange(backs, "ep", 1)
    result = (mixed + sum(back.astype(wide) for back in backs)).astype(narrow)
    arrived = swap_core(result[seqs:])
    return jnp.where(lax.axis_index("ep") % 2 == 0, result[:seqs], arrived)


def solution(mesh):
    placed = (
        P("ep", None),
        P(),
        P("ep", "tp"),
        P("ep", "tp"),
        P("ep", "tp"),
        P("ep", "tp"),
        P("ep", "tp"),
        P("tp"),
        P("ep", "tp", None, None),
        P(),
        P("tp", None),
        P(),
        P("ep", None),
        P("ep"),
        P("ep", None),
        P("ep", None, "tp"),
        P("ep", None, "tp"),
        P("ep", "tp", None),
    )

    return jax.shard_map(
        on_device, mesh=mesh, in_specs=placed, out_specs=P("ep", "tp"), check_vma=False
    )
```
